512 devices in a mesh: grp: 2 (over y), ep: 16 (over z), tp: 16 (over x, core).
Axes of the slice: x: 8, y: 2, z: 16, core: 2. Of those that a mesh axis runs over, the one named last changes fastest.
The devices are a block of a 8x16x16 slice.
Arguments:
- mix_query: bfloat16 [16384, 16, 128], P(('grp', 'ep'), 'tp'), parts along dimension 0, may hold values from -6 to 6
- mix_keys: bfloat16 [16384, 16, 128], P(('grp', 'ep'), 'tp'), parts along dimension 0, may hold values from -6 to 6
- mix_values: bfloat16 [16384, 16, 128], P(('grp', 'ep'), 'tp'), parts along dimension 0, may hold values from -6 to 6
- beta_in: float32 [16, 16384], P('tp', ('grp', 'ep')), parts along dimension 1, may hold values from -9.5 to 6
- decay_in: float32 [16, 16384], P('tp', ('grp', 'ep')), parts along dimension 1, may hold values from -14 to 0
- norm_gain: float32 [128], replicated, may hold values from 0.1 to 1.9
- ffn_input: bfloat16 [4096, 4096], P(('grp', 'ep'), 'tp'), parts along dimension 0, may hold values from -200 to 200
- ffn_gain: float32 [4096], P('tp'), may hold values from 0.1 to 1.9
- expert_ids: int32 [4096, 2], P(('grp', 'ep')), parts along dimension 0, may hold values from 0 to 15, as said below
- expert_share: float32 [4096, 2], P(('grp', 'ep')), parts along dimension 0, may hold values from 0.2 to 1
- w_gate: bfloat16 [16, 4096, 1024], P('ep', None, 'tp'), may hold values from -0.09375 to 0.09375
- w_up: bfloat16 [16, 4096, 1024], P('ep', None, 'tp'), may hold values from -0.09375 to 0.09375
- w_down: bfloat16 [16, 1024, 4096], P('ep', None, 'tp'), may hold values from -0.1875 to 0.1875
Outputs:
- mix_out: bfloat16 [16384, 16, 128], P(('grp', 'ep'), 'tp'), parts along dimension 0
- ffn_out: bfloat16 [4096, 4096], P(('grp', 'ep'), 'tp'), parts along dimension 0
The draws below stay inside these ranges and needn't reach their ends.
There are 2 independent parts, one for each index of `grp`. The reference program is written for one: setup_inputs(seed, part) draws one part's arguments, and reference() takes and returns one part's arrays. A program takes and returns all parts, laid end to end along the dimension named above; an argument that names none is the same for every part. Nothing has to cross between parts.
Inputs may be any that keep to these rules, and one draw needn't show every extreme that they name: `expert_ids`: each row names two different experts of one group, the group being id // 4; the rows of one device (aligned blocks of 128 rows) name every expert exactly 2 * 128 // 16 times.
All inputs are finite; a program needn't handle non-finite values.
Results may differ from the reference program's by a relative error of at most 0.007.
Values may be sent and summed in bfloat16 or wider, within the bound.
A program may use at most 64 MiB of HBM per device.

```python
import math
import jax
import jax.numpy as jnp
from jax import lax

D = 4096
HEADS = 16
HD = 128
BLOCK = 64
SEQ_DEV = 512
SEQUENCE_LENGTH = 8192
FF = 1024
GROUPS = 4
GROUP_SIZE = 4
EXPERTS = 16
RB_EP = 128
TB = 2048


def draw_beta_in(key, part):
    token_sequence = jax.random.split(jax.random.fold_in(key, 11), 2)
    weak_heads = (jax.random.permutation(token_sequence[0], HEADS) < HEADS // 2)[:, None]
    centre = jnp.where(weak_heads, -5.3, 0.0)
    spread = jnp.where(weak_heads, 1.0, 1.5)
    noise = jax.random.truncated_normal(token_sequence[1], -4.0, 4.0, (HEADS, SEQUENCE_LENGTH), jnp.float32)
    return centre + spread * noise


def draw_decay_in(key, part):
    token_sequence = jax.random.split(key, 4)
    head_log_decay = jax.random.uniform(token_sequence[0], (HEADS, 1), jnp.float32, math.log(3e-05), math.log(0.03))
    span_count = 2 * (SEQUENCE_LENGTH // SEQ_DEV)
    span_index = jnp.arange(SEQUENCE_LENGTH) * span_count // SEQUENCE_LENGTH
    span_table = jnp.exp(jax.random.uniform(token_sequence[1], (HEADS, span_count), jnp.float32, math.log(0.5), math.log(2.0)))
    position_values = span_table[:, span_index]
    random_offset = jnp.exp(jax.random.uniform(token_sequence[2], (HEADS, SEQUENCE_LENGTH), jnp.float32, -0.5, 0.5))
    spike_position = jax.random.randint(token_sequence[3], (6,), 0, SEQUENCE_LENGTH)
    spike_tokens = jnp.any(jnp.arange(SEQUENCE_LENGTH)[None, :] == spike_position[:, None], axis=0).astype(jnp.float32)
    decay_rate_rows = jnp.exp(head_log_decay) * position_values * random_offset + 0.4 * spike_tokens[None, :]
    return jnp.log(jnp.expm1(decay_rate_rows))


def draw_ffn_input(key, part):
    token_sequence = jax.random.split(key, 3)
    columns = jnp.arange(D, dtype=jnp.float32) / D
    column_scale = jnp.exp(math.log(3.0) * columns + jax.random.uniform(token_sequence[0], (D,), jnp.float32, -0.4, 0.4))
    base_values = jax.random.truncated_normal(token_sequence[1], -4.0, 4.0, (TB, D), jnp.float32)
    row_scale = jnp.exp(jax.random.uniform(token_sequence[2], (TB, 1), jnp.float32, 0.0, math.log(10.0)))
    return (base_values * row_scale * column_scale[None, :]).astype(jnp.bfloat16)


def draw_expert_ids(key, part):
    source_count = TB // RB_EP
    block_keys = jax.random.split(key, source_count)
    rank_values = jax.vmap(lambda one_key: jax.random.permutation(one_key, RB_EP))(block_keys).reshape(-1)
    group_of = rank_values % GROUPS
    within = rank_values // GROUPS
    first_pick = within % GROUP_SIZE
    second = (first_pick + 1 + within // GROUP_SIZE % (GROUP_SIZE - 1)) % GROUP_SIZE
    return jnp.stack([group_of * GROUP_SIZE + first_pick, group_of * GROUP_SIZE + second], axis=1).astype(jnp.int32)


def block_levels(own_key, shape, pieces, smallest, largest):
    def one(dim, blocks):
        draws = jax.random.uniform(jax.random.fold_in(jax.random.fold_in(own_key, 6), dim), (blocks,), jnp.float32, smallest / len(pieces), largest / len(pieces))
        return jnp.repeat(jnp.exp(draws), shape[dim] // blocks).reshape((-1,) + (1,) * (len(shape) - dim - 1))

    loudness = one(*pieces[0])
    for cut in pieces[1:]:
        loudness = loudness * one(*cut)
    return loudness


def centred(stream_key, shape, scale, bound, cuts=(), held_as=jnp.bfloat16):
    factor_of = block_levels(stream_key, shape, cuts, -0.22, 0.18) if cuts else 1.0
    drawn = jax.random.normal(stream_key, shape, jnp.float32) * scale * factor_of
    return jnp.minimum(jnp.maximum(drawn, -bound), bound).astype(held_as)


def setup_inputs(seed: int = 0, part: int = 0) -> dict:
    streams_of = jax.random.split(jax.random.key(seed), 14)
    part_keys = jax.random.split(jax.random.fold_in(streams_of[13], part), 14)
    return {
        "mix_query": centred(part_keys[0], (SEQUENCE_LENGTH, HEADS, HD), 1.0, 6.0, ((0, 16), (1, 16))),
        "mix_keys": centred(part_keys[1], (SEQUENCE_LENGTH, HEADS, HD), 1.0, 6.0, ((0, 16), (1, 16))),
        "mix_values": centred(part_keys[2], (SEQUENCE_LENGTH, HEADS, HD), 1.0, 6.0, ((0, 16), (1, 16))),
        "beta_in": draw_beta_in(jax.random.fold_in(jax.random.fold_in(streams_of[13], part), 71), part),
        "decay_in": draw_decay_in(jax.random.fold_in(jax.random.fold_in(streams_of[13], part), 71), part),
        "norm_gain": jnp.clip(1.0 + 0.18 * jax.random.normal(streams_of[5], (HD,), jnp.float32), 0.1, 1.9),
        "ffn_input": draw_ffn_input(jax.random.fold_in(jax.random.fold_in(streams_of[13], part), 71), part),
        "ffn_gain": jnp.clip(1.0 + 0.18 * jax.random.normal(streams_of[7], (D,), jnp.float32), 0.1, 1.9),
        "expert_ids": draw_expert_ids(jax.random.fold_in(jax.random.fold_in(streams_of[13], part), 71), part),
        "expert_share": jnp.clip(0.2 + 0.8 * jax.random.uniform(part_keys[9], (TB, 2), jnp.float32) ** block_levels(part_keys[9], (TB, 2), ((0, 16),), -0.2, 0.2), 0.2, 1.0),
        "w_gate": centred(streams_of[10], (EXPERTS, D, FF), D ** -0.5, 0.09375, ((0, 16), (2, 16))),
        "w_up": centred(streams_of[11], (EXPERTS, D, FF), D ** -0.5, 0.09375, ((0, 16), (2, 16))),
        "w_down": centred(streams_of[12], (EXPERTS, FF, D), FF ** -0.5, 0.1875, ((0, 16), (2, 16))),
    }


PRECISE = lax.Precision.HIGHEST
EPSILON = 1e-06

def unit_inverse(strict_lower):
    extent = strict_lower.shape[-1]
    identity = jnp.eye(extent, dtype=jnp.float32)
    powered = -strict_lower
    product = identity + powered
    for section_index in range(1, (extent - 1).bit_length()):
        powered = jnp.matmul(powered, powered, precision=PRECISE)
        product = jnp.matmul(product, identity + powered, precision=PRECISE)
    return product

def block_terms(queries, keyset, valueset, betas, rates):
    extent = queries.shape[-2]
    cumulative = -jnp.cumsum(rates, axis=-1)
    positions = jnp.arange(extent)
    causal = positions[:, None] >= positions[None, :]
    strict = positions[:, None] > positions[None, :]
    spread = cumulative[..., :, None] - cumulative[..., None, :]
    decay_mask = jnp.where(causal, jnp.exp(jnp.where(causal, spread, 0.0)), 0.0)
    keys_beta = keyset * betas[..., None]
    values_beta = valueset * betas[..., None]
    lower_part = jnp.where(strict, jnp.einsum('...id,...jd->...ij', keys_beta, keyset, precision=PRECISE) * decay_mask, 0.0)
    inverse = unit_inverse(lower_part)
    update = jnp.einsum('...ij,...jd->...id', inverse, values_beta, precision=PRECISE)
    correction = jnp.einsum('...ij,...jd->...id', inverse, keys_beta * jnp.exp(cumulative)[..., None], precision=PRECISE)
    scores = jnp.where(causal, jnp.einsum('...id,...jd->...ij', queries, keyset, precision=PRECISE) * decay_mask, 0.0)
    query_decay = queries * jnp.exp(cumulative)[..., None]
    key_decay = keyset * jnp.exp(cumulative[..., -1:] - cumulative)[..., None]
    block_decay = jnp.exp(cumulative[..., -1])
    return (query_decay, key_decay, update, correction, scores, block_decay)

def unit_rows(values_in, factor):
    floats = values_in.astype(jnp.float32)
    return floats * lax.rsqrt(lax.optimization_barrier(jnp.sum(floats * floats, -1, keepdims=True)) + EPSILON) * factor

def mixer_reference(mix_query, mix_keys, mix_values, beta_in, decay_in, norm_gain):
    length, head_count, width = mix_query.shape
    blocks = length // BLOCK

    def to_blocks(tensor):
        return tensor.reshape(blocks, BLOCK, head_count, width).transpose(0, 2, 1, 3)
    queries = to_blocks(unit_rows(mix_query, width ** (-0.5)))
    keyset = to_blocks(unit_rows(mix_keys, 1.0))
    valueset = to_blocks(mix_values.astype(jnp.float32))
    betas = jax.nn.sigmoid(beta_in).reshape(head_count, blocks, BLOCK).transpose(1, 0, 2)
    rates = jax.nn.softplus(decay_in).reshape(head_count, blocks, BLOCK).transpose(1, 0, 2)

    def advance(carried, inputs):
        query_decay, key_decay, update, correction, scores, block_decay = block_terms(*inputs)
        fresh = update - jnp.einsum('hcd,hde->hce', correction, carried, precision=PRECISE)
        output = jnp.einsum('hcd,hde->hce', query_decay, carried, precision=PRECISE) + jnp.einsum('hij,hje->hie', scores, fresh, precision=PRECISE)
        carried = carried * block_decay[:, None, None] + jnp.einsum('hcd,hce->hde', key_decay, fresh, precision=PRECISE)
        return (carried, output)
    initial = jnp.zeros((head_count, width, width), jnp.float32)
    ignored, outputs = lax.scan(advance, initial, (queries, keyset, valueset, betas, rates))
    raw_mix = outputs.transpose(0, 2, 1, 3).reshape(length, head_count, width)
    return (raw_mix * lax.rsqrt(lax.optimization_barrier(jnp.mean(raw_mix * raw_mix, -1, keepdims=True)) + EPSILON) * norm_gain).astype(jnp.bfloat16)

def experts_reference(ffn_input, ffn_gain, expert_ids, expert_share, w_gate, w_up, w_down):
    floats = ffn_input.astype(jnp.float32)
    normed = (floats * lax.rsqrt(lax.optimization_barrier(jnp.mean(floats * floats, -1, keepdims=True)) + EPSILON) * ffn_gain).astype(jnp.bfloat16)
    pick_count = expert_ids.shape[1]
    flat_ids = expert_ids.reshape(-1)
    sort_order = jnp.argsort(flat_ids, stable=True).astype(jnp.int32)
    source_rows = (sort_order // pick_count).reshape(w_gate.shape[0], -1)

    def one_expert(inputs):
        rows_here, gate_weight, up_weight, down_weight = inputs
        chosen = normed[rows_here]
        gate_sum = jnp.dot(chosen, gate_weight, preferred_element_type=jnp.float32)
        up_sum = jnp.dot(chosen, up_weight, preferred_element_type=jnp.float32)
        hidden = (jax.nn.silu(gate_sum) * up_sum).astype(jnp.bfloat16)
        return jnp.dot(hidden, down_weight, preferred_element_type=jnp.float32).astype(jnp.bfloat16)
    copies = lax.map(one_expert, (source_rows, w_gate, w_up, w_down)).reshape(-1, normed.shape[1])
    slots = jnp.argsort(sort_order).astype(jnp.int32)
    per_slot = copies[slots].reshape(expert_ids.shape[0], pick_count, -1)
    return lax.optimization_barrier(jnp.sum(per_slot.astype(jnp.float32) * expert_share[..., None], axis=1)).astype(jnp.bfloat16)

def reference(mix_query, mix_keys, mix_values, beta_in, decay_in, norm_gain, ffn_input, ffn_gain, expert_ids, expert_share, w_gate, w_up, w_down):
    mix_out = mixer_reference(mix_query, mix_keys, mix_values, beta_in, decay_in, norm_gain)
    ffn_out = experts_reference(ffn_input, ffn_gain, expert_ids, expert_share, w_gate, w_up, w_down)
    return (mix_out, ffn_out)
```

```python
import functools

import jax
import jax.numpy as jnp
from jax import lax
from jax.experimental import pallas as pl
from jax.experimental.pallas import tpu as pltpu
from jax.sharding import PartitionSpec as P

MESH = pl.DeviceIdType.MESH
EPSILON = 1e-06
BLOCK = 64
WIDE = 128
F32 = jnp.float32
BF16 = jnp.bfloat16

NN = ((1,), (0,))
NT = ((1,), (1,))
TN = ((0,), (0,))


def dot(a, b, dims=NN):
    return lax.dot_general(a, b, (dims, ((), ())), preferred_element_type=F32)


def halves(a):
    high = a.astype(BF16)
    return high, (a - high.astype(F32)).astype(BF16)


def dot_left(a, b, dims=NN):
    high, low = halves(a)
    return dot(high, b, dims) + dot(low, b, dims)


def dot_right(a, b, dims=NN):
    high, low = halves(b)
    return dot(a, high, dims) + dot(a, low, dims)


def dot_both(a, b, dims=NN):
    ah, al = halves(a)
    bh, bl = halves(b)
    return dot(ah, bh, dims) + (dot(ah, bl, dims) + dot(al, bh, dims))


def down_columns(row):
    return jnp.broadcast_to(row, (row.shape[1], row.shape[1])).T


def grid_of(n):
    return (
        lax.broadcasted_iota(jnp.int32, (n, n), 0),
        lax.broadcasted_iota(jnp.int32, (n, n), 1),
    )


def running_sums(rates):
    i, j = grid_of(WIDE)
    upper = jnp.where(i <= j, 1.0, 0.0).astype(BF16)
    high, rest = halves(rates)
    mid = (rates - high.astype(F32) - rest.astype(F32)).astype(BF16)
    return -(dot(high, upper) + (dot(rest, upper) + dot(mid, upper)))


def group_inverse(q, k, beta, cum):
    i, j = grid_of(WIDE)
    qf, kf = q.astype(F32), k.astype(F32)
    rq = lax.rsqrt(jnp.sum(qf * qf, -1, keepdims=True) + EPSILON) * (WIDE**-0.5)
    rk = lax.rsqrt(jnp.sum(kf * kf, -1, keepdims=True) + EPSILON)
    rk_row = jnp.broadcast_to(rk, (WIDE, WIDE)).T
    spread = jnp.where(i >= j, down_columns(cum) - cum, 0.0)
    decay = jnp.exp(spread) * rk_row
    lower = jnp.where(i > j, dot(k, k, NT) * rk * down_columns(beta) * decay, 0.0)
    scores = jnp.where(i >= j, dot(q, k, NT) * rq * decay, 0.0)
    same = (i // BLOCK) == (j // BLOCK)
    powered = jnp.where(same, -lower, 0.0)
    across = jnp.where(same, 0.0, lower)
    product = jnp.where(i == j, 1.0, 0.0) + powered
    for _ in range(1, (BLOCK - 1).bit_length()):
        powered = dot_both(powered, powered)
        product = product + dot_both(product, powered)
    inverse = product - dot_both(product, dot_both(across, product))
    return inverse, scores, rq, rk, rk_row[:1]


def group_terms(q, k, v, beta, cum, inverse, scores, rq, rk, rk_row):
    i, j = grid_of(WIDE)
    cum_col = down_columns(cum)[:, :1]
    last = cum[:, WIDE - 1 :]
    update = dot_left(inverse * beta, v)
    correction = dot_left(inverse * (beta * jnp.exp(cum) * rk_row), k)
    both = jnp.concatenate([update, correction], axis=1)
    moved = dot_right(k, both * (rk * jnp.exp(last - cum_col)), TN)
    shift = moved[:, :WIDE]
    transfer = jnp.where(i == j, jnp.exp(last), 0.0) - moved[:, WIDE:]
    seen = dot_both(scores, both)
    base = seen[:, :WIDE]
    reach = q.astype(F32) * (rq * jnp.exp(cum_col)) - seen[:, WIDE:]
    return shift, transfer, base, reach


def softplus(x):
    return jnp.maximum(x, 0.0) + jnp.log1p(jnp.exp(-jnp.abs(x)))


def dispatch_tables(ids, capacity, experts):
    tokens = ids.shape[1]
    lane = lax.broadcasted_iota(jnp.int32, (tokens, WIDE), 1)
    first = jnp.broadcast_to(ids[0:1].astype(F32), (tokens, tokens)).T.astype(jnp.int32)[:, :WIDE]
    second = jnp.broadcast_to(ids[1:2].astype(F32), (tokens, tokens)).T.astype(jnp.int32)[:, :WIDE]
    one = jnp.where(lane == first, 1.0, 0.0)
    two = jnp.where(lane == second, 1.0, 0.0)
    i, j = grid_of(tokens)
    before = jnp.where(i > j, 1.0, 0.0).astype(BF16)
    rank = dot(before, (one + two).astype(BF16)) + (lane * capacity).astype(F32)
    slot_one = jnp.sum(one * rank, -1, keepdims=True).astype(jnp.int32)
    slot_two = jnp.sum(two * rank, -1, keepdims=True).astype(jnp.int32)
    return slot_one, slot_two


def program_kernel(nz, nx, *refs):
    (
        q_in, k_in, v_in, beta_in, decay_in, ng_in, x_in, gain_in, ids_in, share_in,
        wg_in, wu_in, wd_in, mix_out, ffn_out,
        q_s, k_s, v_s, beta_s, decay_s, ng_s, x_s, gains, ids_s, share_s, wt, wd,
        rows_s, xs, xg, hg, ret, got, comm, base_s, reach_s, qm, sf, sb, mo_s, fo_s,
        load_sem, disp_send, disp_recv, x_send, x_recv, hid_send, hid_recv,
        ret_send, ret_recv, g_send, g_recv, w_send, w_recv, f_send, f_recv, b_send, b_recv,
    ) = refs
    grp, z, tp = lax.axis_index("grp"), lax.axis_index("ep"), lax.axis_index("tp")
    x, c = tp // 2, tp % 2
    partner = 2 * x + 1 - c
    tokens, feats = x_s.shape
    capacity = xs.shape[1]
    hid = wg_in.shape[0]
    groups = q_s.shape[0] // WIDE
    sources = nz // 2
    parity = z % 2
    mine = z // 2
    waits = []

    def remote(src, dst, send, recv, zz, tt):
        return pltpu.make_async_remote_copy(
            src_ref=src, dst_ref=dst, send_sem=send, recv_sem=recv,
            device_id=(grp, zz, tt), device_id_type=MESH,
        )

    barrier = pltpu.get_barrier_semaphore()
    for dz in sorted(range(1, nz), key=lambda k: -min(k, nz - k)):
        for core in range(2):
            pl.semaphore_signal(
                barrier, inc=1, device_id=(grp, (z + dz) % nz, 2 * x + core), device_id_type=MESH
            )
    for dt in range(1, 2 * nx):
        pl.semaphore_signal(
            barrier, inc=1, device_id=(grp, z, (tp + dt) % (2 * nx)), device_id_type=MESH
        )

    places = [
        (x_in, x_s), (ids_in, ids_s), (beta_in, beta_s), (decay_in, decay_s), (k_in, k_s), (q_in, q_s),
        (v_in, v_s), (gain_in, gains.at[tp]), (share_in, share_s), (ng_in, ng_s),
        (wg_in, wt.at[pl.ds(pl.multiple_of(c * hid, hid), hid), :]),
        (wu_in, wt.at[pl.ds(pl.multiple_of((2 + c) * hid, hid), hid), :]),
        (wd_in, wd.at[c]),
    ]
    loads = [pltpu.make_async_copy(src, dst, load_sem.at[n]) for n, (src, dst) in enumerate(places)]
    for load in loads:
        load.start()

    loads[0].wait()
    loads[1].wait()
    slot_one, slot_two = dispatch_tables(ids_s[...], capacity, nz)
    slots = lax.broadcasted_iota(jnp.int32, (tokens, 2 * tokens), 1)
    chosen = jnp.where((slots == slot_one) | (slots == slot_two), 1.0, 0.0).astype(BF16)
    ordered = dot(chosen, x_s[...], TN).astype(BF16)
    for e in range(nz):
        xs[e] = ordered[e * capacity : (e + 1) * capacity]

    for n in (2, 3, 4, 5):
        loads[n].wait()
    for g in range(groups):
        cut = slice(g * WIDE, (g + 1) * WIDE)
        rows_s[0, g : g + 1, :] = 1.0 / (1.0 + jnp.exp(-beta_s[:, cut]))
        rows_s[1, g : g + 1, :] = softplus(decay_s[:, cut])
    for g in range(groups, 8):
        rows_s[1, g : g + 1, :] = jnp.zeros((1, WIDE), F32)
    rows_s[2] = running_sums(rows_s[1])
    firsts = []
    for g in range(groups):
        cut = slice(g * WIDE, (g + 1) * WIDE)
        beta, cum = rows_s[0, g : g + 1, :], rows_s[2, g : g + 1, :]
        firsts.append(group_inverse(q_s[cut], k_s[cut], beta, cum))

    pl.semaphore_wait(barrier, 2 * (nz - 1) + 2 * nx - 1)

    row_here = pl.ds(pl.multiple_of(mine * capacity, capacity), capacity)
    for dz in sorted(range(1, nz), key=lambda k: -min(k, nz - k)):
        e = (z + dz) % nz
        copy = remote(
            xs.at[e], xg.at[x, c, row_here, :], disp_send.at[dz], disp_recv.at[mine, c], e, 2 * x + parity
        )
        copy.start()
        waits.append((None, copy))
    own = remote(xs.at[z], xg.at[x, c, row_here, :], disp_send.at[0], disp_recv.at[mine, c], z, partner)

    @pl.when(parity != c)
    def _():
        own.start()

    waits.append((parity != c, own))

    @pl.when(parity == c)
    def _():
        xg[x, c, row_here, :] = xs[z]

    loads[7].wait()
    for dt in range(1, 2 * nx):
        copy = remote(gains.at[tp], gains.at[tp], g_send.at[dt], g_recv.at[dt], z, (tp + dt) % (2 * nx))
        copy.start()
        waits.append((None, copy))
    to_partner = []
    for n, (src, dst) in enumerate(places[10:]):
        copy = remote(src, dst, w_send.at[n], w_recv.at[n], z, partner)
        copy.start()
        waits.append((None, copy))
        to_partner.append(copy)

    loads[6].wait()
    total = None
    for g in range(groups):
        cut = slice(g * WIDE, (g + 1) * WIDE)
        beta, cum = rows_s[0, g : g + 1, :], rows_s[2, g : g + 1, :]
        shift, transfer, base, reach = group_terms(q_s[cut], k_s[cut], v_s[cut], beta, cum, *firsts[g])
        if total is None:
            total = jnp.concatenate([shift, transfer], axis=1)
        else:
            through = dot_both(reach, total)
            base = base + through[:, :WIDE]
            reach = through[:, WIDE:]
            total = dot_both(transfer, total)
            total = jnp.concatenate([total[:, :WIDE] + shift, total[:, WIDE:]], axis=1)
        base_s[cut, :] = base
        reach_s[cut, :] = reach
    comm[z] = total.astype(BF16)
    i, j = grid_of(WIDE)
    qm[...] = jnp.where(i == j, 1.0, 0.0)
    sf[...] = jnp.zeros_like(sf)
    sb[...] = jnp.zeros_like(sb)
    ahead = nz // 2
    behind = nz - 1 - ahead
    wrapped = nz - 1 - ahead

    def pass_forward(step, owner, condition):
        copy = remote(comm.at[owner], comm.at[owner], f_send.at[step], f_recv.at[step], (z + 1) % nz, tp)

        @pl.when(condition)
        def _():
            copy.start()

        waits.append((condition, copy))

    def pass_backward(step, owner, condition):
        copy = remote(
            comm.at[owner], comm.at[owner], b_send.at[step], b_recv.at[step], (z + nz - 1) % nz, tp
        )

        @pl.when(condition)
        def _():
            copy.start()

        waits.append((condition, copy))

    pass_forward(1, z, z + 1 < nz)
    pass_backward(1, z, z < wrapped)

    def map_step(d):
        if d <= ahead:
            owner = (z + nz - d) % nz
            fits = z >= d
            arrival = remote(
                comm.at[owner], comm.at[owner], f_send.at[d], f_recv.at[d], (z + 1) % nz, tp
            )

            @pl.when(fits)
            def _():
                arrival.wait_recv()

            if d < ahead:
                pass_forward(d + 1, owner, jnp.logical_and(fits, z + 1 < nz))

        if d <= behind:
            owner_back = (z + d) % nz
            fits_back = owner_back < wrapped
            arrival_back = remote(
                comm.at[owner_back], comm.at[owner_back], b_send.at[d], b_recv.at[d], (z + 1) % nz, tp
            )

            @pl.when(fits_back)
            def _():
                arrival_back.wait_recv()

            if d < behind:
                pass_backward(d + 1, owner_back, fits_back)

        if d <= ahead:

            @pl.when(fits)
            def _():
                advanced = dot_left(qm[...], comm[owner])
                sf[...] += advanced[:, :WIDE]
                qm[...] = advanced[:, WIDE:]

        if d <= behind:

            @pl.when(jnp.logical_and(fits_back, z + d >= nz))
            def _():
                message = comm[owner_back]
                sb[...] = dot_right(message[:, WIDE:], sb[...]) + message[:, :WIDE].astype(F32)

    pieces = min(4, sources)
    per_piece = sources // pieces
    piece_rows = per_piece * capacity
    distance = nx // 2
    order = [0] + [o for k in range(1, pieces) for o in (k, pieces - k) if k <= pieces - k]
    order = list(dict.fromkeys(order))
    where = [(z // (2 * per_piece) + o) % pieces for o in order]

    def piece_of(chip, n):
        rows = pl.ds(pl.multiple_of(where[n] * piece_rows, piece_rows), piece_rows)
        return xg.at[chip, :, rows, :]

    def travels(way, d):
        if d < distance:
            return range(pieces)
        return range(pieces // 2) if way == 0 else range(pieces // 2, pieces)

    def ring(way, d, n):
        chip = (x + nx - (d - 1)) % nx if way == 0 else (x + d - 1) % nx
        to = (x + 1) % nx if way == 0 else (x + nx - 1) % nx
        return remote(
            piece_of(chip, n), piece_of(chip, n), x_send.at[way, d, n], x_recv.at[way, d, n], z, 2 * to + c
        )

    def arrived(way, d, n):
        chip = (x + nx - d) % nx if way == 0 else (x + d) % nx
        to = (x + 1) % nx if way == 0 else (x + nx - 1) % nx
        return remote(
            piece_of(chip, n), piece_of(chip, n), x_send.at[way, d, n], x_recv.at[way, d, n], z, 2 * to + c
        )

    for n in range(pieces):
        for t in range(per_piece):
            m = where[n] * per_piece + t
            for core in range(2):
                rows = pl.ds(pl.multiple_of(m * capacity, capacity), capacity)
                landing = xg.at[x, core, rows, :]
                arrival = remote(landing, landing, disp_send.at[0], disp_recv.at[m, core], z, partner)

                @pl.when(jnp.logical_or(2 * m + c != z, core != c))
                def _():
                    arrival.wait_recv()

        for way in range(2):
            if n in travels(way, 1):
                copy = ring(way, 1, n)
                copy.start()
                waits.append((None, copy))

    for load in loads[8:]:
        load.wait()
    for n in range(3):
        to_partner[n].wait_recv()
    for dt in range(1, 2 * nx):
        sender = (tp + 2 * nx - dt) % (2 * nx)
        remote(gains.at[sender], gains.at[sender], g_send.at[dt], g_recv.at[dt], z, sender).wait_recv()

    def products(chip, acc, squares):
        for core in range(2):
            part = xg[chip, core].astype(F32)
            squares = squares + jnp.sum(part * part, -1, keepdims=True)
            member = 2 * chip + core
            scaled = (part * gains[member]).astype(BF16)
            columns = pl.ds(pl.multiple_of(member * feats, feats), feats)
            acc = acc + dot(scaled, wt[:, columns], NT)
        return acc, squares

    rows_all = sources * capacity
    acc = jnp.zeros((rows_all, 4 * hid), F32)
    squares = jnp.zeros((rows_all, 1), F32)
    acc, squares = products(x, acc, squares)
    for d in range(1, distance + 1):
        for n in range(pieces):
            for way in range(2):
                if n in travels(way, d):
                    arrived(way, d, n).wait_recv()
                    if d < distance and n in travels(way, d + 1):
                        copy = ring(way, d + 1, n)
                        copy.start()
                        waits.append((None, copy))
        map_step(d)
        acc, squares = products((x + nx - d) % nx, acc, squares)
        if d < distance:
            acc, squares = products((x + d) % nx, acc, squares)

    scale = lax.rsqrt(squares / (feats * 2 * nx) + EPSILON)
    gate = acc[:, : 2 * hid] * scale
    up = acc[:, 2 * hid :] * scale
    hg[x] = (gate / (1.0 + jnp.exp(-gate)) * up).astype(BF16)
    for dx in sorted(range(1, nx), key=lambda k: -min(k, nx - k)):
        copy = remote(hg.at[x], hg.at[x], hid_send.at[dx], hid_recv.at[dx], z, 2 * ((x + dx) % nx) + c)
        copy.start()
        waits.append((None, copy))
    done = distance
    for d in range(done + 1, min(done + 3, ahead + 1)):
        map_step(d)
        done = d
    for dx in range(1, nx):
        chip = (x + nx - dx) % nx
        remote(hg.at[chip], hg.at[chip], hid_send.at[dx], hid_recv.at[dx], z, 2 * chip + c).wait_recv()
    hidden = jnp.concatenate([hg[n] for n in range(nx)], axis=1)
    for core in range(2):
        ret[core] = dot(hidden, wd[core]).astype(BF16)

    slot_here = pl.ds(pl.multiple_of(z * capacity, capacity), capacity)
    for dm in sorted(range(sources), key=lambda k: -min(k, sources - k)):
        m = (mine + dm) % sources
        rows = pl.ds(pl.multiple_of(m * capacity, capacity), capacity)
        target = 2 * m + c
        for core in range(2):
            copy = remote(
                ret.at[core, rows, :], got.at[slot_here, :], ret_send.at[dm, core], ret_recv.at[z],
                target, 2 * x + core,
            )
            away = jnp.logical_or(target != z, core != c)

            @pl.when(away)
            def _():
                copy.start()

            waits.append((away, copy))

            @pl.when(jnp.logical_not(away))
            def _():
                got[slot_here, :] = ret[core, rows, :]

    for d in range(done + 1, ahead + 1):
        map_step(d)
    entering = sf[...] + dot_both(qm[...], sb[...])
    for g in range(groups):
        cut = slice(g * WIDE, (g + 1) * WIDE)
        raw = base_s[cut, :] + dot_both(reach_s[cut, :], entering)
        norm = lax.rsqrt(jnp.mean(raw * raw, -1, keepdims=True) + EPSILON)
        mo_s[cut, :] = (raw * norm * ng_s[...]).astype(BF16)
    store_mix = pltpu.make_async_copy(mo_s, mix_out, load_sem.at[13])
    store_mix.start()

    shares = share_s[...]
    first = jnp.broadcast_to(shares[0:1], (tokens, tokens)).T[:, :1]
    second = jnp.broadcast_to(shares[1:2], (tokens, tokens)).T[:, :1]
    weights = jnp.where(slots == slot_one, first, 0.0) + jnp.where(slots == slot_two, second, 0.0)
    for e in range(nz):
        landing = got.at[pl.ds(e * capacity, capacity), :]
        arrival = remote(landing, landing, disp_send.at[0], ret_recv.at[e], z, partner)

        @pl.when(jnp.logical_or(e != z, parity != c))
        def _():
            arrival.wait_recv()

    fo_s[...] = dot_left(weights, got[...]).astype(BF16)
    store_ffn = pltpu.make_async_copy(fo_s, ffn_out, load_sem.at[14])
    store_ffn.start()
    for condition, copy in waits:
        if condition is None:
            copy.wait_send()
        else:

            @pl.when(condition)
            def _():
                copy.wait_send()

    store_mix.wait()
    store_ffn.wait()


def body(nz, nx, mix_query, mix_keys, mix_values, beta_in, decay_in, norm_gain, ffn_input, ffn_gain,
         expert_ids, expert_share, w_gate, w_up, w_down):
    length, _, width = mix_query.shape
    tokens, feats = ffn_input.shape
    hid = w_gate.shape[2]
    full = w_gate.shape[1]
    capacity = 2 * tokens // nz
    rows = nz // 2 * capacity
    ff = w_down.shape[1]
    dma = pltpu.SemaphoreType.DMA
    vmem = pltpu.VMEM
    call = pl.pallas_call(
        functools.partial(program_kernel, nz, nx),
        out_shape=(
            jax.ShapeDtypeStruct((length, width), BF16),
            jax.ShapeDtypeStruct((tokens, feats), BF16),
        ),
        in_specs=[pl.BlockSpec(memory_space=pl.ANY)] * 13,
        out_specs=[pl.BlockSpec(memory_space=pl.ANY)] * 2,
        scratch_shapes=[
            vmem((length, width), BF16), vmem((length, width), BF16), vmem((length, width), BF16),
            vmem((1, length), F32), vmem((1, length), F32), vmem((1, width), F32),
            vmem((tokens, feats), BF16), vmem((2 * nx, 1, feats), F32),
            vmem((2, tokens), jnp.int32), vmem((2, tokens), F32),
            vmem((4 * hid, full), BF16), vmem((2, ff, feats), BF16),
            vmem((3, 8, width), F32),
            vmem((nz, capacity, feats), BF16),
            vmem((nx, 2, rows, feats), BF16),
            vmem((nx, rows, 2 * hid), BF16),
            vmem((2, rows, feats), BF16),
            vmem((2 * tokens, feats), BF16),
            vmem((nz, width, 2 * width), BF16),
            vmem((length, width), F32), vmem((length, width), F32),
            vmem((width, width), F32), vmem((width, width), F32), vmem((width, width), F32),
            vmem((length, width), BF16), vmem((tokens, feats), BF16),
            dma((15,)), dma((nz,)), dma((nz // 2, 2)),
            dma((2, nx // 2 + 1, 4)), dma((2, nx // 2 + 1, 4)),
            dma((nx,)), dma((nx,)),
            dma((nz // 2, 2)), dma((nz,)),
            dma((2 * nx,)), dma((2 * nx,)), dma((3,)), dma((3,)),
            dma((nz // 2 + 1,)), dma((nz // 2 + 1,)), dma((nz // 2 + 1,)), dma((nz // 2 + 1,)),
        ],
        compiler_params=pltpu.CompilerParams(collective_id=0, has_side_effects=True),
    )
    mix, ffn = call(
        mix_query.reshape(length, width), mix_keys.reshape(length, width), mix_values.reshape(length, width),
        beta_in, decay_in, norm_gain.reshape(1, width), ffn_input, ffn_gain.reshape(1, feats),
        expert_ids.T, expert_share.T, w_gate[0].T, w_up[0].T, w_down[0],
    )
    return mix.reshape(length, 1, width), ffn


def solution(mesh):
    nz, nx = mesh.shape["ep"], mesh.shape["tp"] // 2
    in_specs = (
        P(("grp", "ep"), "tp", None), P(("grp", "ep"), "tp", None), P(("grp", "ep"), "tp", None),
        P("tp", ("grp", "ep")), P("tp", ("grp", "ep")), P(),
        P(("grp", "ep"), "tp"), P("tp"), P(("grp", "ep"), None), P(("grp", "ep"), None),
        P("ep", None, "tp"), P("ep", None, "tp"), P("ep", None, "tp"),
    )
    out_specs = (P(("grp", "ep"), "tp", None), P(("grp", "ep"), "tp"))
    return jax.shard_map(
        functools.partial(body, nz, nx), mesh=mesh, in_specs=in_specs, out_specs=out_specs, check_vma=False
    )
```

```python
import functools

import jax
import jax.numpy as jnp
from jax import lax
from jax.experimental import pallas as pl
from jax.experimental.pallas import tpu as pltpu
from jax.sharding import PartitionSpec as P

MESH = pl.DeviceIdType.MESH
EPSILON = 1e-06
BLOCK = 64
WIDE = 128
F32 = jnp.float32
BF16 = jnp.bfloat16

NN = ((1,), (0,))
NT = ((1,), (1,))
TN = ((0,), (0,))


def dot(a, b, dims=NN):
    return lax.dot_general(a, b, (dims, ((), ())), preferred_element_type=F32)


def halves(a):
    high = a.astype(BF16)
    return high, (a - high.astype(F32)).astype(BF16)


def dot_left(a, b, dims=NN):
    high, low = halves(a)
    return dot(high, b, dims) + dot(low, b, dims)


def dot_right(a, b, dims=NN):
    high, low = halves(b)
    return dot(a, high, dims) + dot(a, low, dims)


def dot_both(a, b, dims=NN):
    ah, al = halves(a)
    bh, bl = halves(b)
    return dot(ah, bh, dims) + (dot(ah, bl, dims) + dot(al, bh, dims))


def down_columns(row):
    return jnp.broadcast_to(row, (row.shape[1], row.shape[1])).T


def grid_of(n):
    return (
        lax.broadcasted_iota(jnp.int32, (n, n), 0),
        lax.broadcasted_iota(jnp.int32, (n, n), 1),
    )


def running_sums(rates):
    i, j = grid_of(WIDE)
    upper = jnp.where(i <= j, 1.0, 0.0).astype(BF16)
    high, rest = halves(rates)
    mid = (rates - high.astype(F32) - rest.astype(F32)).astype(BF16)
    return -(dot(high, upper) + (dot(rest, upper) + dot(mid, upper)))


def group_inverse(q, k, beta, cum):
    i, j = grid_of(WIDE)
    qf, kf = q.astype(F32), k.astype(F32)
    rq = lax.rsqrt(jnp.sum(qf * qf, -1, keepdims=True) + EPSILON) * (WIDE**-0.5)
    rk = lax.rsqrt(jnp.sum(kf * kf, -1, keepdims=True) + EPSILON)
    rk_row = jnp.broadcast_to(rk, (WIDE, WIDE)).T
    spread = jnp.where(i >= j, down_columns(cum) - cum, 0.0)
    decay = jnp.exp(spread) * rk_row
    lower = jnp.where(i > j, dot(k, k, NT) * rk * down_columns(beta) * decay, 0.0)
    scores = jnp.where(i >= j, dot(q, k, NT) * rq * decay, 0.0)
    same = (i // BLOCK) == (j // BLOCK)
    powered = jnp.where(same, -lower, 0.0)
    across = jnp.where(same, 0.0, lower)
    product = jnp.where(i == j, 1.0, 0.0) + powered
    for _ in range(1, (BLOCK - 1).bit_length()):
        powered = dot_both(powered, powered)
        product = product + dot_both(product, powered)
    inverse = product - dot_both(product, dot_both(across, product))
    return inverse, scores, rq, rk, rk_row[:1]


def group_terms(q, k, v, beta, cum, inverse, scores, rq, rk, rk_row):
    i, j = grid_of(WIDE)
    cum_col = down_columns(cum)[:, :1]
    last = cum[:, WIDE - 1 :]
    update = dot_left(inverse * beta, v)
    correction = dot_left(inverse * (beta * jnp.exp(cum) * rk_row), k)
    both = jnp.concatenate([update, correction], axis=1)
    moved = dot_right(k, both * (rk * jnp.exp(last - cum_col)), TN)
    shift = moved[:, :WIDE]
    transfer = jnp.where(i == j, jnp.exp(last), 0.0) - moved[:, WIDE:]
    seen = dot_both(scores, both)
    base = seen[:, :WIDE]
    reach = q.astype(F32) * (rq * jnp.exp(cum_col)) - seen[:, WIDE:]
    return shift, transfer, base, reach


def softplus(x):
    return jnp.maximum(x, 0.0) + jnp.log1p(jnp.exp(-jnp.abs(x)))


def dispatch_tables(ids, capacity, experts):
    tokens = ids.shape[1]
    lane = lax.broadcasted_iota(jnp.int32, (tokens, WIDE), 1)
    first = jnp.broadcast_to(ids[0:1].astype(F32), (tokens, tokens)).T.astype(jnp.int32)[:, :WIDE]
    second = jnp.broadcast_to(ids[1:2].astype(F32), (tokens, tokens)).T.astype(jnp.int32)[:, :WIDE]
    one = jnp.where(lane == first, 1.0, 0.0)
    two = jnp.where(lane == second, 1.0, 0.0)
    i, j = grid_of(tokens)
    before = jnp.where(i > j, 1.0, 0.0).astype(BF16)
    rank = dot(before, (one + two).astype(BF16)) + (lane * capacity).astype(F32)
    slot_one = jnp.sum(one * rank, -1, keepdims=True).astype(jnp.int32)
    slot_two = jnp.sum(two * rank, -1, keepdims=True).astype(jnp.int32)
    return slot_one, slot_two


def program_kernel(nz, nx, *refs):
    (
        q_in, k_in, v_in, beta_in, decay_in, ng_in, x_in, gain_in, ids_in, share_in,
        wg_in, wu_in, wd_in, mix_out, ffn_out,
        q_s, k_s, v_s, beta_s, decay_s, ng_s, x_s, gains, ids_s, share_s, wt, wd,
        rows_s, xs, xg, hg, ret, got, base_s, reach_s, total_s, state_in, state_out, mo_s, fo_s,
        load_sem, ready, disp_send, disp_recv, x_send, x_recv, hid_send, hid_recv,
        ret_send, ret_recv, g_send, g_recv, w_send, w_recv, s_send, s_recv,
    ) = refs
    grp, z, tp = lax.axis_index("grp"), lax.axis_index("ep"), lax.axis_index("tp")
    x, c = tp // 2, tp % 2
    partner = 2 * x + 1 - c
    tokens, feats = x_s.shape
    capacity = xs.shape[1]
    hid = wg_in.shape[0]
    groups = q_s.shape[0] // WIDE
    sources = nz // 2
    parity = z % 2
    mine = z // 2
    early = z < nz // 2
    first = z < nz // 4
    waits = []

    def remote(src, dst, send, recv, zz, tt):
        return pltpu.make_async_remote_copy(
            src_ref=src, dst_ref=dst, send_sem=send, recv_sem=recv,
            device_id=(grp, zz, tt), device_id_type=MESH,
        )

    def hop(k):
        return min(k, nz - k)

    places = [
        (x_in, x_s), (ids_in, ids_s), (beta_in, beta_s), (decay_in, decay_s), (k_in, k_s), (q_in, q_s),
        (v_in, v_s), (gain_in, gains.at[tp]), (share_in, share_s), (ng_in, ng_s),
        (wg_in, wt.at[pl.ds(pl.multiple_of(c * hid, hid), hid), :]),
        (wu_in, wt.at[pl.ds(pl.multiple_of((2 + c) * hid, hid), hid), :]),
        (wd_in, wd.at[c]),
    ]
    loads = [pltpu.make_async_copy(src, dst, load_sem.at[n]) for n, (src, dst) in enumerate(places)]
    for load in loads:
        load.start()

    barrier = pltpu.get_barrier_semaphore()
    for dt in sorted(range(1, 2 * nx), key=lambda k: -min(k, 2 * nx - k)):
        pl.semaphore_signal(
            barrier, inc=1, device_id=(grp, z, (tp + dt) % (2 * nx)), device_id_type=MESH
        )
    for k in range(1, nz):

        @pl.when(z + k < nz)
        def _():
            for core in range(2):
                pl.semaphore_signal(
                    barrier, inc=1, device_id=(grp, (z + k) % nz, 2 * x + core), device_id_type=MESH
                )

    def mixer_blocks():
        for g in range(groups):
            cut = slice(g * WIDE, (g + 1) * WIDE)
            rows_s[0, g : g + 1, :] = 1.0 / (1.0 + jnp.exp(-beta_s[:, cut]))
            rows_s[1, g : g + 1, :] = softplus(decay_s[:, cut])
        for g in range(groups, 8):
            rows_s[1, g : g + 1, :] = jnp.zeros((1, WIDE), F32)
        rows_s[2] = running_sums(rows_s[1])
        total = None
        for g in range(groups):
            cut = slice(g * WIDE, (g + 1) * WIDE)
            beta, cum = rows_s[0, g : g + 1, :], rows_s[2, g : g + 1, :]
            inverse = group_inverse(q_s[cut], k_s[cut], beta, cum)
            shift, transfer, base, reach = group_terms(q_s[cut], k_s[cut], v_s[cut], beta, cum, *inverse)
            if total is None:
                total = jnp.concatenate([shift, transfer], axis=1)
            else:
                through = dot_both(reach, total)
                base = base + through[:, :WIDE]
                reach = through[:, WIDE:]
                total = dot_both(transfer, total)
                total = jnp.concatenate([total[:, :WIDE] + shift, total[:, WIDE:]], axis=1)
            base_s[cut, :] = base
            reach_s[cut, :] = reach
        total_s[...] = total

    for n in range(2, 7):
        loads[n].wait()

    @pl.when(early)
    def _():
        mixer_blocks()

    pl.semaphore_wait(barrier, 2 * nx - 1 + 2 * z)

    for k in range(nz - 1, 0, -1):

        @pl.when(z >= k)
        def _():
            for core in range(2):
                pl.semaphore_signal(
                    ready.at[z], inc=1, device_id=(grp, (z + nz - k) % nz, 2 * x + core), device_id_type=MESH
                )

    loads[0].wait()
    loads[1].wait()
    slot_one, slot_two = dispatch_tables(ids_s[...], capacity, nz)
    slots = lax.broadcasted_iota(jnp.int32, (tokens, 2 * tokens), 1)
    chosen = jnp.where((slots == slot_one) | (slots == slot_two), 1.0, 0.0).astype(BF16)
    ordered = dot(chosen, x_s[...], TN).astype(BF16)
    for e in range(nz):
        xs[e] = ordered[e * capacity : (e + 1) * capacity]

    row_here = pl.ds(pl.multiple_of(mine * capacity, capacity), capacity)

    def rows_to(e):
        return remote(
            xs.at[e], xg.at[x, c, row_here, :], disp_send.at[e], disp_recv.at[mine, c], e, 2 * x + parity
        )

    for k in sorted(range(1, nz), key=lambda k: -hop(k)):

        @pl.when(z >= k)
        def _():
            rows_to((z + nz - k) % nz).start()

        waits.append((None, rows_to((z + k) % nz)))
    own = remote(xs.at[z], xg.at[x, c, row_here, :], disp_send.at[z], disp_recv.at[mine, c], z, partner)

    @pl.when(parity != c)
    def _():
        own.start()

    waits.append((parity != c, own))

    @pl.when(parity == c)
    def _():
        xg[x, c, row_here, :] = xs[z]

    loads[7].wait()
    for dt in range(1, 2 * nx):
        copy = remote(gains.at[tp], gains.at[tp], g_send.at[dt], g_recv.at[dt], z, (tp + dt) % (2 * nx))
        copy.start()
        waits.append((None, copy))
    to_partner = []
    for n, (src, dst) in enumerate(places[10:]):
        copy = remote(src, dst, w_send.at[n], w_recv.at[n], z, partner)
        copy.start()
        waits.append((None, copy))
        to_partner.append(copy)

    def ready_step(k, condition):
        e = (z + k) % nz

        @pl.when(jnp.logical_and(z + k < nz, condition))
        def _():
            pl.semaphore_wait(ready.at[e], 2)
            rows_to(e).start()

    cuts = [0]
    while cuts[-1] < sources:
        cuts.append(min(max(1, 2 * cuts[-1]), sources))
    pieces = len(cuts) - 1

    def span(n):
        return slice(cuts[n] * capacity, cuts[n + 1] * capacity)

    def features(chip, n, dx):
        part = xg.at[chip, :, pl.ds(cuts[n] * capacity, (cuts[n + 1] - cuts[n]) * capacity), :]
        return remote(part, part, x_send.at[dx, n], x_recv.at[dx, n], z, 2 * ((x + dx) % nx) + c)

    def hidden_of(chip, n, dx):
        part = hg.at[chip, pl.ds(cuts[n] * capacity, (cuts[n + 1] - cuts[n]) * capacity), :]
        return remote(part, part, hid_send.at[dx, n], hid_recv.at[dx, n], z, 2 * ((x + dx) % nx) + c)

    farthest = sorted(range(1, nx), key=lambda k: -min(k, nx - k))

    def gather_rows(n):
        for m in range(cuts[n], cuts[n + 1]):
            for core in range(2):
                landing = xg.at[x, core, pl.ds(m * capacity, capacity), :]
                arrival = remote(landing, landing, disp_send.at[0], disp_recv.at[m, core], z, partner)

                @pl.when(jnp.logical_or(2 * m + c != z, core != c))
                def _():
                    arrival.wait_recv()

        for dx in farthest:
            copy = features(x, n, dx)
            copy.start()
            waits.append((None, copy))

    def make_hidden(n):
        for dx in range(1, nx):
            features((x + nx - dx) % nx, n, dx).wait_recv()
        count = (cuts[n + 1] - cuts[n]) * capacity
        acc = jnp.zeros((count, 4 * hid), F32)
        squares = jnp.zeros((count, 1), F32)
        for member in range(2 * nx):
            part = xg[member // 2, member % 2, span(n), :].astype(F32)
            squares = squares + jnp.sum(part * part, -1, keepdims=True)
            scaled = (part * gains[member]).astype(BF16)
            acc = acc + dot(scaled, wt[:, member * feats : (member + 1) * feats], NT)
        scale = lax.rsqrt(squares / (feats * 2 * nx) + EPSILON)
        gate = acc[:, : 2 * hid] * scale
        up = acc[:, 2 * hid :] * scale
        hg[x, span(n), :] = (gate / (1.0 + jnp.exp(-gate)) * up).astype(BF16)
        for dx in farthest:
            copy = hidden_of(x, n, dx)
            copy.start()
            waits.append((None, copy))

    slot_here = pl.ds(pl.multiple_of(z * capacity, capacity), capacity)

    def give_back(n):
        for dx in range(1, nx):
            hidden_of((x + nx - dx) % nx, n, dx).wait_recv()
        hidden = jnp.concatenate([hg[chip, span(n), :] for chip in range(nx)], axis=1)
        for core in range(2):
            ret[core, span(n), :] = dot(hidden, wd[core]).astype(BF16)
        for m in range(cuts[n], cuts[n + 1]):
            target = 2 * m + c
            rows = pl.ds(m * capacity, capacity)
            for core in range(2):
                copy = remote(
                    ret.at[core, rows, :], got.at[slot_here, :], ret_send.at[m, core], ret_recv.at[z],
                    target, 2 * x + core,
                )
                away = jnp.logical_or(target != z, core != c)

                @pl.when(away)
                def _():
                    copy.start()

                waits.append((away, copy))

                @pl.when(jnp.logical_not(away))
                def _():
                    got[slot_here, :] = ret[core, rows, :]

    store_mix = pltpu.make_async_copy(mo_s, mix_out, load_sem.at[13])
    state = remote(state_out, state_in, s_send.at[0], s_recv.at[0], (z + 1) % nz, tp)

    def pass_state():
        @pl.when(z > 0)
        def _():
            state.wait_recv()

        @pl.when(z == 0)
        def _():
            state_in[...] = jnp.zeros_like(state_in)

        entering = state_in[...]

        @pl.when(z + 1 < nz)
        def _():
            leaving = dot_left(total_s[:, WIDE:], entering) + total_s[:, :WIDE]
            state_out[...] = leaving.astype(BF16)
            state.start()

        for g in range(groups):
            cut = slice(g * WIDE, (g + 1) * WIDE)
            raw = base_s[cut, :] + dot_left(reach_s[cut, :], entering)
            norm = lax.rsqrt(jnp.mean(raw * raw, -1, keepdims=True) + EPSILON)
            mo_s[cut, :] = (raw * norm * ng_s[...]).astype(BF16)
        store_mix.start()

    waits.append((z + 1 < nz, state))

    def weights_here():
        for load in loads[8:]:
            load.wait()
        for n in range(3):
            to_partner[n].wait_recv()
        for dt in range(1, 2 * nx):
            sender = (tp + 2 * nx - dt) % (2 * nx)
            remote(gains.at[sender], gains.at[sender], g_send.at[dt], g_recv.at[dt], z, sender).wait_recv()

    for k in range(1, nz):
        ready_step(k, first)
    after = jnp.logical_not(first)
    steps = iter(range(1, nz))

    def ready_steps(count):
        for k in [k for _, k in zip(range(count), steps)]:
            ready_step(k, after)

    ready_steps(1)
    gather_rows(0)
    ready_steps(2)
    if pieces > 1:
        gather_rows(1)
    weights_here()
    make_hidden(0)
    ready_steps(2)
    if pieces > 1:
        make_hidden(1)
    give_back(0)
    ready_steps(3)
    if pieces > 1:
        give_back(1)

    @pl.when(jnp.logical_not(early))
    def _():
        mixer_blocks()

    ready_steps(nz)
    for n in range(2, pieces):
        gather_rows(n)
    for n in range(2, pieces):
        make_hidden(n)
        give_back(n)
        if n == 2:

            @pl.when(early)
            def _():
                pass_state()

    if pieces < 3:

        @pl.when(early)
        def _():
            pass_state()

    @pl.when(jnp.logical_not(early))
    def _():
        pass_state()

    shares = share_s[...]
    first_share = jnp.broadcast_to(shares[0:1], (tokens, tokens)).T[:, :1]
    second_share = jnp.broadcast_to(shares[1:2], (tokens, tokens)).T[:, :1]
    weights = jnp.where(slots == slot_one, first_share, 0.0) + jnp.where(slots == slot_two, second_share, 0.0)
    for e in range(nz):
        landing = got.at[pl.ds(e * capacity, capacity), :]
        arrival = remote(landing, landing, disp_send.at[0], ret_recv.at[e], z, partner)

        @pl.when(jnp.logical_or(e != z, parity != c))
        def _():
            arrival.wait_recv()

    fo_s[...] = dot_left(weights, got[...]).astype(BF16)
    store_ffn = pltpu.make_async_copy(fo_s, ffn_out, load_sem.at[14])
    store_ffn.start()
    for condition, copy in waits:
        if condition is None:
            copy.wait_send()
        else:

            @pl.when(condition)
            def _():
                copy.wait_send()

    store_mix.wait()
    store_ffn.wait()


def body(nz, nx, mix_query, mix_keys, mix_values, beta_in, decay_in, norm_gain, ffn_input, ffn_gain,
         expert_ids, expert_share, w_gate, w_up, w_down):
    length, _, width = mix_query.shape
    tokens, feats = ffn_input.shape
    hid = w_gate.shape[2]
    full = w_gate.shape[1]
    capacity = 2 * tokens // nz
    rows = nz // 2 * capacity
    ff = w_down.shape[1]
    dma = pltpu.SemaphoreType.DMA
    vmem = pltpu.VMEM
    call = pl.pallas_call(
        functools.partial(program_kernel, nz, nx),
        out_shape=(
            jax.ShapeDtypeStruct((length, width), BF16),
            jax.ShapeDtypeStruct((tokens, feats), BF16),
        ),
        in_specs=[pl.BlockSpec(memory_space=pl.ANY)] * 13,
        out_specs=[pl.BlockSpec(memory_space=pl.ANY)] * 2,
        scratch_shapes=[
            vmem((length, width), BF16), vmem((length, width), BF16), vmem((length, width), BF16),
            vmem((1, length), F32), vmem((1, length), F32), vmem((1, width), F32),
            vmem((tokens, feats), BF16), vmem((2 * nx, 1, feats), F32),
            vmem((2, tokens), jnp.int32), vmem((2, tokens), F32),
            vmem((4 * hid, full), BF16), vmem((2, ff, feats), BF16),
            vmem((3, 8, width), F32),
            vmem((nz, capacity, feats), BF16),
            vmem((nx, 2, rows, feats), BF16),
            vmem((nx, rows, 2 * hid), BF16),
            vmem((2, rows, feats), BF16),
            vmem((2 * tokens, feats), BF16),
            vmem((length, width), F32), vmem((length, width), F32), vmem((width, 2 * width), F32),
            vmem((width, width), BF16), vmem((width, width), BF16),
            vmem((length, width), BF16), vmem((tokens, feats), BF16),
            dma((15,)), pltpu.SemaphoreType.REGULAR((nz,)), dma((nz,)), dma((nz // 2, 2)),
            dma((nx, 4)), dma((nx, 4)), dma((nx, 4)), dma((nx, 4)),
            dma((nz // 2, 2)), dma((nz,)),
            dma((2 * nx,)), dma((2 * nx,)), dma((3,)), dma((3,)), dma((1,)), dma((1,)),
        ],
        compiler_params=pltpu.CompilerParams(collective_id=0, has_side_effects=True),
    )
    mix, ffn = call(
        mix_query.reshape(length, width), mix_keys.reshape(length, width), mix_values.reshape(length, width),
        beta_in, decay_in, norm_gain.reshape(1, width), ffn_input, ffn_gain.reshape(1, feats),
        expert_ids.T, expert_share.T, w_gate[0].T, w_up[0].T, w_down[0],
    )
    return mix.reshape(length, 1, width), ffn


def solution(mesh):
    nz, nx = mesh.shape["ep"], mesh.shape["tp"] // 2
    in_specs = (
        P(("grp", "ep"), "tp", None), P(("grp", "ep"), "tp", None), P(("grp", "ep"), "tp", None),
        P("tp", ("grp", "ep")), P("tp", ("grp", "ep")), P(),
        P(("grp", "ep"), "tp"), P("tp"), P(("grp", "ep"), None), P(("grp", "ep"), None),
        P("ep", None, "tp"), P("ep", None, "tp"), P("ep", None, "tp"),
    )
    out_specs = (P(("grp", "ep"), "tp", None), P(("grp", "ep"), "tp"))
    return jax.shard_map(
        functools.partial(body, nz, nx), mesh=mesh, in_specs=in_specs, out_specs=out_specs, check_vma=False
    )
```

```python
import functools

import jax
import jax.numpy as jnp
from jax import lax
from jax.experimental import pallas as pl
from jax.experimental.pallas import tpu as pltpu
from jax.sharding import PartitionSpec as P

MESH = pl.DeviceIdType.MESH
EPSILON = 1e-06
BLOCK = 64
WIDE = 128
F32 = jnp.float32
BF16 = jnp.bfloat16

NN = ((1,), (0,))
NT = ((1,), (1,))
TN = ((0,), (0,))


def dot(a, b, dims=NN):
    return lax.dot_general(a, b, (dims, ((), ())), preferred_element_type=F32)


def halves(a):
    high = a.astype(BF16)
    return high, (a - high.astype(F32)).astype(BF16)


def dot_left(a, b, dims=NN):
    high, low = halves(a)
    return dot(high, b, dims) + dot(low, b, dims)


def dot_right(a, b, dims=NN):
    high, low = halves(b)
    return dot(a, high, dims) + dot(a, low, dims)


def dot_both(a, b, dims=NN):
    ah, al = halves(a)
    bh, bl = halves(b)
    return dot(ah, bh, dims) + (dot(ah, bl, dims) + dot(al, bh, dims))


def down_columns(row):
    return jnp.broadcast_to(row, (row.shape[1], row.shape[1])).T


def grid_of(n):
    return (
        lax.broadcasted_iota(jnp.int32, (n, n), 0),
        lax.broadcasted_iota(jnp.int32, (n, n), 1),
    )


def running_sums(rates):
    i, j = grid_of(WIDE)
    upper = jnp.where(i <= j, 1.0, 0.0).astype(BF16)
    high, rest = halves(rates)
    mid = (rates - high.astype(F32) - rest.astype(F32)).astype(BF16)
    return -(dot(high, upper) + (dot(rest, upper) + dot(mid, upper)))


def group_inverses(qs, ks, betas, cums):
    i, j = grid_of(WIDE)
    same = (i // BLOCK) == (j // BLOCK)
    each = range(len(qs))
    rqs, rks, scores, lowers = [], [], [], []
    for q, k, beta, cum in zip(qs, ks, betas, cums):
        qf, kf = q.astype(F32), k.astype(F32)
        rq = lax.rsqrt(jnp.sum(qf * qf, -1, keepdims=True) + EPSILON) * (WIDE**-0.5)
        rk = lax.rsqrt(jnp.sum(kf * kf, -1, keepdims=True) + EPSILON)
        rk_row = jnp.broadcast_to(rk, (WIDE, WIDE)).T
        spread = jnp.where(i >= j, down_columns(cum) - cum, 0.0)
        decay = jnp.exp(spread) * rk_row
        lowers.append(jnp.where(i > j, dot(k, k, NT) * rk * down_columns(beta) * decay, 0.0))
        scores.append(jnp.where(i >= j, dot(q, k, NT) * rq * decay, 0.0))
        rqs.append(rq)
        rks.append((rk, rk_row[:1]))
    powered = [jnp.where(same, -lowers[g], 0.0) for g in each]
    product = [jnp.where(i == j, 1.0, 0.0) + powered[g] for g in each]
    for _ in range(1, (BLOCK - 1).bit_length()):
        powered = [dot_both(powered[g], powered[g]) for g in each]
        product = [product[g] + dot_both(product[g], powered[g]) for g in each]
    crossed = [dot_both(jnp.where(same, 0.0, lowers[g]), product[g]) for g in each]
    inverses = [product[g] - dot_both(product[g], crossed[g]) for g in each]
    return [(inverses[g], scores[g], rqs[g], *rks[g]) for g in each]


def group_terms(q, k, v, beta, cum, inverse, scores, rq, rk, rk_row):
    i, j = grid_of(WIDE)
    cum_col = down_columns(cum)[:, :1]
    last = cum[:, WIDE - 1 :]
    update = dot_left(inverse * beta, v)
    correction = dot_left(inverse * (beta * jnp.exp(cum) * rk_row), k)
    both = jnp.concatenate([update, correction], axis=1)
    moved = dot_right(k, both * (rk * jnp.exp(last - cum_col)), TN)
    shift = moved[:, :WIDE]
    transfer = jnp.where(i == j, jnp.exp(last), 0.0) - moved[:, WIDE:]
    seen = dot_both(scores, both)
    base = seen[:, :WIDE]
    reach = q.astype(F32) * (rq * jnp.exp(cum_col)) - seen[:, WIDE:]
    return shift, transfer, base, reach


def softplus(x):
    return jnp.maximum(x, 0.0) + jnp.log1p(jnp.exp(-jnp.abs(x)))


def dispatch_tables(ids, capacity, experts):
    tokens = ids.shape[1]
    lane = lax.broadcasted_iota(jnp.int32, (tokens, WIDE), 1)
    first = jnp.broadcast_to(ids[0:1].astype(F32), (tokens, tokens)).T.astype(jnp.int32)[:, :WIDE]
    second = jnp.broadcast_to(ids[1:2].astype(F32), (tokens, tokens)).T.astype(jnp.int32)[:, :WIDE]
    one = jnp.where(lane == first, 1.0, 0.0)
    two = jnp.where(lane == second, 1.0, 0.0)
    i, j = grid_of(tokens)
    before = jnp.where(i > j, 1.0, 0.0).astype(BF16)
    rank = dot(before, (one + two).astype(BF16)) + (lane * capacity).astype(F32)
    slot_one = jnp.sum(one * rank, -1, keepdims=True).astype(jnp.int32)
    slot_two = jnp.sum(two * rank, -1, keepdims=True).astype(jnp.int32)
    return slot_one, slot_two


def program_kernel(nz, nx, *refs):
    (
        q_in, k_in, v_in, beta_in, decay_in, ng_in, x_in, gain_in, ids_in, share_in,
        wg_in, wu_in, wd_in, mix_out, ffn_out,
        q_s, k_s, v_s, beta_s, decay_s, ng_s, x_s, gains, ids_s, share_s, wt, wd,
        rows_s, xs, xg, hg, ret, got, base_s, reach_s, total_s, map_out, map_in, state_in, state_out, parts_s, mo_s, fo_s,
        load_sem, ready, disp_send, disp_recv, x_send, x_recv, hid_send, hid_recv,
        ret_send, ret_recv, g_send, g_recv, w_send, w_recv, s_send, s_recv, m_send, m_recv,
    ) = refs
    grp, z, tp = lax.axis_index("grp"), lax.axis_index("ep"), lax.axis_index("tp")
    x, c = tp // 2, tp % 2
    partner = 2 * x + 1 - c
    tokens, feats = x_s.shape
    capacity = xs.shape[1]
    hid = wg_in.shape[0]
    groups = q_s.shape[0] // WIDE
    sources = nz // 2
    parity = z % 2
    mine = z // 2
    first = z < nz // 4
    corner = jnp.logical_and(z == 0, tp == 0)
    usual = jnp.logical_not(corner)
    below = jnp.logical_and(z > 0, x == 0)
    beside = jnp.logical_and(z == 0, tp > 0)
    early = jnp.logical_and(z < nz // 2, usual)
    waits = []

    def remote(src, dst, send, recv, zz, tt):
        return pltpu.make_async_remote_copy(
            src_ref=src, dst_ref=dst, send_sem=send, recv_sem=recv,
            device_id=(grp, zz, tt), device_id_type=MESH,
        )

    def hop(k):
        return min(k, nz - k)

    barrier = pltpu.get_barrier_semaphore()

    def greet(sem, zz, tt):
        pl.semaphore_signal(sem, inc=1, device_id=(grp, zz, tt), device_id_type=MESH)

    around = sorted(range(1, 2 * nx), key=lambda k: -min(k, 2 * nx - k))

    @pl.when(below)
    def _():
        greet(barrier, 0, 0)

    @pl.when(usual)
    def _():
        for dt in around:
            greet(barrier, z, (tp + dt) % (2 * nx))

    for k in range(1, nz):

        @pl.when(jnp.logical_and(z + k < nz, usual))
        def _():
            for core in range(2):
                greet(barrier, (z + k) % nz, 2 * x + core)

    places = [
        (x_in, x_s), (ids_in, ids_s), (beta_in, beta_s), (decay_in, decay_s), (k_in, k_s), (q_in, q_s),
        (v_in, v_s), (gain_in, gains.at[tp]), (share_in, share_s), (ng_in, ng_s),
        (wg_in, wt.at[pl.ds(pl.multiple_of(c * hid, hid), hid), :]),
        (wu_in, wt.at[pl.ds(pl.multiple_of((2 + c) * hid, hid), hid), :]),
        (wd_in, wd.at[c]),
    ]
    loads = [pltpu.make_async_copy(src, dst, load_sem.at[n]) for n, (src, dst) in enumerate(places)]
    for load in loads:
        load.start()

    def mixer_blocks():
        for g in range(groups):
            cut = slice(g * WIDE, (g + 1) * WIDE)
            rows_s[0, g : g + 1, :] = 1.0 / (1.0 + jnp.exp(-beta_s[:, cut]))
            rows_s[1, g : g + 1, :] = softplus(decay_s[:, cut])
        for g in range(groups, 8):
            rows_s[1, g : g + 1, :] = jnp.zeros((1, WIDE), F32)
        rows_s[2] = running_sums(rows_s[1])
        cuts = [slice(g * WIDE, (g + 1) * WIDE) for g in range(groups)]
        qs, ks, vs = [q_s[cut] for cut in cuts], [k_s[cut] for cut in cuts], [v_s[cut] for cut in cuts]
        betas = [rows_s[0, g : g + 1, :] for g in range(groups)]
        cums = [rows_s[2, g : g + 1, :] for g in range(groups)]
        inverses = group_inverses(qs, ks, betas, cums)
        terms = [group_terms(qs[g], ks[g], vs[g], betas[g], cums[g], *inverses[g]) for g in range(groups)]
        total = None
        for cut, (shift, transfer, base, reach) in zip(cuts, terms):
            if total is None:
                total = jnp.concatenate([shift, transfer], axis=1)
            else:
                through = dot_both(reach, total)
                base = base + through[:, :WIDE]
                reach = through[:, WIDE:]
                total = dot_both(transfer, total)
                total = jnp.concatenate([total[:, :WIDE] + shift, total[:, WIDE:]], axis=1)
            base_s[cut, :] = base
            reach_s[cut, :] = reach
        total_s[...] = total
        map_out[...] = total.astype(BF16)

    loads[0].wait()
    loads[1].wait()
    slot_one, slot_two = dispatch_tables(ids_s[...], capacity, nz)
    slots = lax.broadcasted_iota(jnp.int32, (tokens, 2 * tokens), 1)
    chosen = jnp.where((slots == slot_one) | (slots == slot_two), 1.0, 0.0).astype(BF16)
    ordered = dot(chosen, x_s[...], TN).astype(BF16)
    for e in range(nz):
        xs[e] = ordered[e * capacity : (e + 1) * capacity]

    for n in range(2, 7):
        loads[n].wait()

    @pl.when(early)
    def _():
        mixer_blocks()

    missing = jnp.where(jnp.logical_or(below, beside), 1, 0)
    pl.semaphore_wait(barrier, 2 * nx - 1 + jnp.where(corner, 2 * (nz - 1), 2 * z - missing))

    for k in range(nz - 1, 0, -1):

        @pl.when(z >= k)
        def _():
            @pl.when(jnp.logical_or(z > k, x > 0))
            def _():
                greet(ready.at[z], (z + nz - k) % nz, 2 * x)

            greet(ready.at[z], (z + nz - k) % nz, 2 * x + 1)

    row_here = pl.ds(pl.multiple_of(mine * capacity, capacity), capacity)

    def rows_to(e):
        return remote(
            xs.at[e], xg.at[x, c, row_here, :], disp_send.at[e], disp_recv.at[mine, c], e, 2 * x + parity
        )

    for k in sorted(range(1, nz), key=lambda k: -hop(k)):
        to_corner = jnp.logical_and(z == k, jnp.logical_and(x == 0, parity == 0))

        @pl.when(jnp.logical_or(corner, jnp.logical_and(z >= k, jnp.logical_not(to_corner))))
        def _():
            rows_to((z + nz - k) % nz).start()

        waits.append((None, rows_to((z + k) % nz)))

    @pl.when(corner)
    def _():
        for dt in around:
            greet(ready.at[0], z, (tp + dt) % (2 * nx))
        for k in range(1, nz):
            for core in range(2):
                greet(ready.at[0], (z + k) % nz, 2 * x + core)

    own = remote(xs.at[z], xg.at[x, c, row_here, :], disp_send.at[z], disp_recv.at[mine, c], z, partner)
    own_away = jnp.logical_and(beside, tp == 1)

    @pl.when(jnp.logical_and(parity != c, jnp.logical_not(own_away)))
    def _():
        own.start()

    waits.append((parity != c, own))

    @pl.when(parity == c)
    def _():
        xg[x, c, row_here, :] = xs[z]

    loads[7].wait()

    def gains_to(dt):
        return remote(gains.at[tp], gains.at[tp], g_send.at[dt], g_recv.at[dt], z, (tp + dt) % (2 * nx))

    for dt in range(1, 2 * nx):

        @pl.when(jnp.logical_or(z > 0, (tp + dt) % (2 * nx) > 0))
        def _():
            gains_to(dt).start()

        waits.append((None, gains_to(dt)))
    to_partner = [remote(src, dst, w_send.at[n], w_recv.at[n], z, partner) for n, (src, dst) in enumerate(places[10:])]

    @pl.when(jnp.logical_not(own_away))
    def _():
        for copy in to_partner:
            copy.start()

    for copy in to_partner:
        waits.append((None, copy))

    @pl.when(corner)
    def _():
        mixer_blocks()

    def ready_step(k, condition):
        e = (z + k) % nz

        @pl.when(jnp.logical_and(z + k < nz, condition))
        def _():
            pl.semaphore_wait(ready.at[e], 2)
            rows_to(e).start()

    def block(ref, lead, begin, end):
        return ref.at[lead, pl.ds(begin * capacity, (end - begin) * capacity), :]

    def features(chip, begin, end, sem, dx):
        part = xg.at[chip, :, pl.ds(begin * capacity, (end - begin) * capacity), :]
        return remote(part, part, x_send.at[dx, sem], x_recv.at[dx, sem], z, 2 * ((x + dx) % nx) + c)

    def hidden_of(chip, begin, end, sem, dx):
        part = block(hg, chip, begin, end)
        return remote(part, part, hid_send.at[dx, sem], hid_recv.at[dx, sem], z, 2 * ((x + dx) % nx) + c)

    farthest = sorted(range(1, nx), key=lambda k: -min(k, nx - k))
    branch = [None]
    gathered = []

    def started(make, *at):
        make(*at).start()
        waits.append((branch[0], functools.partial(make, *at)))

    def meet_corner(spans=()):
        @pl.when(jnp.logical_or(below, beside))
        def _():
            pl.semaphore_wait(ready.at[0], 1)

            @pl.when(jnp.logical_and(below, parity == 0))
            def _():
                rows_to(0).start()

        if spans:

            @pl.when(beside)
            def _():
                gains_to(2 * nx - tp).start()

                @pl.when(tp == 1)
                def _():
                    own.start()
                    for copy in to_partner:
                        copy.start()

                @pl.when(c == 0)
                def _():
                    for n, (b, e) in enumerate(spans):
                        features(x, b, e, n, nx - x).start()

    def gather_rows(begin, end, sem, skip_corner=False, condition=None):
        def go():
            for m in range(begin, end):
                for core in range(2):
                    landing = xg.at[x, core, pl.ds(m * capacity, capacity), :]
                    arrival = remote(landing, landing, disp_send.at[0], disp_recv.at[m, core], z, partner)

                    @pl.when(jnp.logical_or(2 * m + c != z, core != c))
                    def _():
                        arrival.wait_recv()

            for dx in farthest:
                skipped = jnp.logical_and(jnp.logical_and(z == 0, c == 0), (x + dx) % nx == 0)

                @pl.when(jnp.logical_not(jnp.logical_and(skipped, skip_corner)))
                def _():
                    features(x, begin, end, sem, dx).start()

        if condition is None:
            go()
        else:
            pl.when(condition)(go)
        if (begin, end, sem, branch[0] is first) not in gathered:
            gathered.append((begin, end, sem, branch[0] is first))
            for dx in farthest:
                waits.append((branch[0], functools.partial(features, x, begin, end, sem, dx)))

    def make_hidden(begin, end, parts, sem):
        for first_row, last_row, part_sem in parts:
            for dx in range(1, nx):
                features((x + nx - dx) % nx, first_row, last_row, part_sem, dx).wait_recv()
        rows = slice(begin * capacity, end * capacity)
        acc = jnp.zeros(((end - begin) * capacity, 4 * hid), F32)
        squares = jnp.zeros(((end - begin) * capacity, 1), F32)
        for member in range(2 * nx):
            part = xg[member // 2, member % 2, rows, :].astype(F32)
            squares = squares + jnp.sum(part * part, -1, keepdims=True)
            scaled = (part * gains[member]).astype(BF16)
            acc = acc + dot(scaled, wt[:, member * feats : (member + 1) * feats], NT)
        scale = lax.rsqrt(squares / (feats * 2 * nx) + EPSILON)
        gate = acc[:, : 2 * hid] * scale
        up = acc[:, 2 * hid :] * scale
        hg[x, rows, :] = (gate / (1.0 + jnp.exp(-gate)) * up).astype(BF16)
        for dx in farthest:
            started(hidden_of, x, begin, end, sem, dx)

    slot_here = pl.ds(pl.multiple_of(z * capacity, capacity), capacity)

    def result(m, core):
        return remote(
            ret.at[core, pl.ds(m * capacity, capacity), :], got.at[slot_here, :],
            ret_send.at[m, core], ret_recv.at[z], 2 * m + c, 2 * x + core,
        )

    def away(m, core):
        return jnp.logical_or(2 * m + c != z, core != c)

    def give_back(begin, end, sem):
        for dx in range(1, nx):
            hidden_of((x + nx - dx) % nx, begin, end, sem, dx).wait_recv()
        rows = slice(begin * capacity, end * capacity)
        hidden = jnp.concatenate([hg[chip, rows, :] for chip in range(nx)], axis=1)
        for core in range(2):
            ret[core, rows, :] = dot(hidden, wd[core]).astype(BF16)
        for m in range(begin, end):
            for core in range(2):

                @pl.when(away(m, core))
                def _():
                    result(m, core).start()

                @pl.when(jnp.logical_not(away(m, core)))
                def _():
                    got[slot_here, :] = ret[core, m * capacity : (m + 1) * capacity, :]

    for m in range(sources):
        for core in range(2):
            waits.append((away(m, core), result(m, core)))

    store_mix = pltpu.make_async_copy(mo_s, mix_out, load_sem.at[13])
    odd = z % 2 == 1
    send_map = jnp.logical_and(jnp.logical_not(odd), z + 1 < nz)
    own_map = remote(map_out, map_in, m_send.at[0], m_recv.at[0], (z + 1) % nz, tp)
    state_near = remote(state_out, state_in, s_send.at[0], s_recv.at[0], (z + 1) % nz, tp)
    state_far = remote(state_out, state_in, s_send.at[1], s_recv.at[0], (z + 2) % nz, tp)
    waits.append((send_map, own_map))
    waits.append((jnp.logical_and(odd, z + 1 < nz), state_near))
    waits.append((jnp.logical_and(odd, z + 2 < nz), state_far))

    def pass_map(condition):
        @pl.when(jnp.logical_and(condition, send_map))
        def _():
            own_map.start()

    def pass_state():
        @pl.when(z > 1)
        def _():
            state_near.wait_recv()

        @pl.when(z <= 1)
        def _():
            state_in[...] = jnp.zeros_like(state_in)

        @pl.when(odd)
        def _():
            own_map.wait_recv()
            before = map_in[...]
            entering = dot_right(before[:, WIDE:], state_in[...].astype(F32)) + before[:, :WIDE].astype(F32)
            leaving = dot_both(total_s[:, WIDE:], entering) + total_s[:, :WIDE]
            state_out[...] = leaving.astype(BF16)
            high, low = halves(entering)
            parts_s[0] = high
            parts_s[1] = low

            @pl.when(z + 2 < nz)
            def _():
                state_far.start()

            @pl.when(z + 1 < nz)
            def _():
                state_near.start()

        @pl.when(jnp.logical_not(odd))
        def _():
            parts_s[0] = state_in[...]
            parts_s[1] = jnp.zeros_like(state_in)

        for g in range(groups):
            cut = slice(g * WIDE, (g + 1) * WIDE)
            high, low = halves(reach_s[cut, :])
            across = dot(high, parts_s[1]) + dot(low, parts_s[0])
            raw = base_s[cut, :] + (dot(high, parts_s[0]) + across)
            norm = lax.rsqrt(jnp.mean(raw * raw, -1, keepdims=True) + EPSILON)
            mo_s[cut, :] = (raw * norm * ng_s[...]).astype(BF16)
        store_mix.start()

    def weights_here():
        for load in loads[8:]:
            load.wait()
        for n in range(3):
            to_partner[n].wait_recv()
        for dt in range(1, 2 * nx):
            sender = (tp + 2 * nx - dt) % (2 * nx)
            remote(gains.at[sender], gains.at[sender], g_send.at[dt], g_recv.at[dt], z, sender).wait_recv()

    def marks(*fractions):
        found = [0]
        for part, whole in fractions:
            found.append(max(found[-1], sources * part // whole))
        found.append(sources)
        return [(b, e) for b, e in zip(found[:-1], found[1:]) if e > b]

    branch[0] = first

    @pl.when(first)
    def _():
        steps = iter(range(1, nz))

        def ready_steps(count):
            for k in [k for _, k in zip(range(count), steps)]:
                ready_step(k, usual)

        spans = marks((1, 4), (2, 4), (3, 4), (7, 8))
        last_span = len(spans) - 1
        ready_steps(1)
        pass_map(first)
        ready_steps(nz // 4 - 1)
        waiting = jnp.logical_and(below, c == 0)
        before, later = list(enumerate(spans[:-1]))[:2], list(enumerate(spans[:-1]))[2:]
        for n, (b, e) in before:
            gather_rows(b, e, n, True, jnp.logical_not(waiting) if n == 0 else None)
            ready_steps(nz // 4 if n == 0 else nz // 8)
        meet_corner(spans[: len(before)])
        gather_rows(*spans[0], 0, False, waiting)
        ready_steps(nz // 8)
        for n, (b, e) in later:
            gather_rows(b, e, n)
            ready_steps(1)
        ready_steps(nz)
        weights_here()
        bulk = spans[last_span][0]
        half = spans[min(2, last_span)][0]
        inner = [(b, e, n) for n, (b, e) in enumerate(spans)]
        parts = [(b, e) for b, e in ((0, half), (half, bulk), (bulk, sources)) if e > b]
        given = 0
        for n, (b, e) in enumerate(parts):
            if n == len(parts) - 1 and n > 1:
                give_back(*parts[0], 0)
                given = 1
            make_hidden(b, e, [p for p in inner if b <= p[0] < e], n)
            if n == 0:
                gather_rows(bulk, sources, last_span)
        for n in range(given, len(parts)):
            give_back(*parts[n], n)

    after = jnp.logical_not(first)
    branch[0] = after

    @pl.when(after)
    def _():
        steps = iter(range(1, nz))

        def ready_steps(count):
            for k in [k for _, k in zip(range(count), steps)]:
                ready_step(k, usual)

        spans = marks((1, 8), (2, 8), (4, 8), (6, 8))
        count = len(spans)

        def gather(n):
            if n < count:
                gather_rows(*spans[n], n)

        def hide(n):
            if n < count:
                make_hidden(*spans[n], [(*spans[n], n)], n)

        def give(n):
            if n < count:
                give_back(*spans[n], n)

        ready_steps(1)
        pass_map(early)
        meet_corner()
        gather(0)
        ready_steps(2)
        gather(1)
        ready_steps(nz)
        weights_here()
        hide(0)
        hide(1)
        gather(2)
        give(0)
        give(1)
        hide(2)
        gather(3)
        give(2)
        gather(4)
        for n in range(3, count):
            hide(n)
        for n in range(3, count):
            give(n)

    @pl.when(z >= nz // 2)
    def _():
        mixer_blocks()

    pass_map(z >= nz // 2)
    pass_state()

    shares = share_s[...]
    first_share = jnp.broadcast_to(shares[0:1], (tokens, tokens)).T[:, :1]
    second_share = jnp.broadcast_to(shares[1:2], (tokens, tokens)).T[:, :1]
    weights = jnp.where(slots == slot_one, first_share, 0.0) + jnp.where(slots == slot_two, second_share, 0.0)
    for e in range(nz):
        landing = got.at[pl.ds(e * capacity, capacity), :]
        arrival = remote(landing, landing, disp_send.at[0], ret_recv.at[e], z, partner)

        @pl.when(jnp.logical_or(e != z, parity != c))
        def _():
            arrival.wait_recv()

    fo_s[...] = dot_left(weights, got[...]).astype(BF16)
    store_ffn = pltpu.make_async_copy(fo_s, ffn_out, load_sem.at[14])
    store_ffn.start()
    for condition, copy in waits:

        def settle():
            (copy() if callable(copy) else copy).wait_send()

        if condition is None:
            settle()
        else:
            pl.when(condition)(settle)

    store_mix.wait()
    store_ffn.wait()


def body(nz, nx, mix_query, mix_keys, mix_values, beta_in, decay_in, norm_gain, ffn_input, ffn_gain,
         expert_ids, expert_share, w_gate, w_up, w_down):
    length, _, width = mix_query.shape
    tokens, feats = ffn_input.shape
    hid = w_gate.shape[2]
    full = w_gate.shape[1]
    capacity = 2 * tokens // nz
    rows = nz // 2 * capacity
    ff = w_down.shape[1]
    dma = pltpu.SemaphoreType.DMA
    vmem = pltpu.VMEM
    call = pl.pallas_call(
        functools.partial(program_kernel, nz, nx),
        out_shape=(
            jax.ShapeDtypeStruct((length, width), BF16),
            jax.ShapeDtypeStruct((tokens, feats), BF16),
        ),
        in_specs=[pl.BlockSpec(memory_space=pl.ANY)] * 13,
        out_specs=[pl.BlockSpec(memory_space=pl.ANY)] * 2,
        scratch_shapes=[
            vmem((length, width), BF16), vmem((length, width), BF16), vmem((length, width), BF16),
            vmem((1, length), F32), vmem((1, length), F32), vmem((1, width), F32),
            vmem((tokens, feats), BF16), vmem((2 * nx, 1, feats), F32),
            vmem((2, tokens), jnp.int32), vmem((2, tokens), F32),
            vmem((4 * hid, full), BF16), vmem((2, ff, feats), BF16),
            vmem((3, 8, width), F32),
            vmem((nz, capacity, feats), BF16),
            vmem((nx, 2, rows, feats), BF16),
            vmem((nx, rows, 2 * hid), BF16),
            vmem((2, rows, feats), BF16),
            vmem((2 * tokens, feats), BF16),
            vmem((length, width), F32), vmem((length, width), F32), vmem((width, 2 * width), F32),
            vmem((width, 2 * width), BF16), vmem((width, 2 * width), BF16),
            vmem((width, width), BF16), vmem((width, width), BF16), vmem((2, width, width), BF16),
            vmem((length, width), BF16), vmem((tokens, feats), BF16),
            dma((15,)), pltpu.SemaphoreType.REGULAR((nz,)), dma((nz,)), dma((nz // 2, 2)),
            dma((nx, 5)), dma((nx, 5)), dma((nx, 5)), dma((nx, 5)),
            dma((nz // 2, 2)), dma((nz,)),
            dma((2 * nx,)), dma((2 * nx,)), dma((3,)), dma((3,)), dma((2,)), dma((1,)), dma((1,)), dma((1,)),
        ],
        compiler_params=pltpu.CompilerParams(collective_id=0, has_side_effects=True),
    )
    mix, ffn = call(
        mix_query.reshape(length, width), mix_keys.reshape(length, width), mix_values.reshape(length, width),
        beta_in, decay_in, norm_gain.reshape(1, width), ffn_input, ffn_gain.reshape(1, feats),
        expert_ids.T, expert_share.T, w_gate[0].T, w_up[0].T, w_down[0],
    )
    return mix.reshape(length, 1, width), ffn


def solution(mesh):
    nz, nx = mesh.shape["ep"], mesh.shape["tp"] // 2
    in_specs = (
        P(("grp", "ep"), "tp", None), P(("grp", "ep"), "tp", None), P(("grp", "ep"), "tp", None),
        P("tp", ("grp", "ep")), P("tp", ("grp", "ep")), P(),
        P(("grp", "ep"), "tp"), P("tp"), P(("grp", "ep"), None), P(("grp", "ep"), None),
        P("ep", None, "tp"), P("ep", None, "tp"), P("ep", None, "tp"),
    )
    out_specs = (P(("grp", "ep"), "tp", None), P(("grp", "ep"), "tp"))
    return jax.shard_map(
        functools.partial(body, nz, nx), mesh=mesh, in_specs=in_specs, out_specs=out_specs, check_vma=False
    )
```

```python
import functools

import jax
import jax.numpy as jnp
from jax import lax
from jax.experimental import pallas as pl
from jax.experimental.pallas import tpu as pltpu
from jax.sharding import PartitionSpec as P

MESH = pl.DeviceIdType.MESH
EPSILON = 1e-06
BLOCK = 64
WIDE = 128
F32 = jnp.float32
BF16 = jnp.bfloat16

NN = ((1,), (0,))
NT = ((1,), (1,))
TN = ((0,), (0,))


def dot(a, b, dims=NN):
    return lax.dot_general(a, b, (dims, ((), ())), preferred_element_type=F32)


def halves(a):
    high = a.astype(BF16)
    return high, (a - high.astype(F32)).astype(BF16)


def dot_left(a, b, dims=NN):
    high, low = halves(a)
    return dot(high, b, dims) + dot(low, b, dims)


def dot_right(a, b, dims=NN):
    high, low = halves(b)
    return dot(a, high, dims) + dot(a, low, dims)


def dot_both(a, b, dims=NN):
    ah, al = halves(a)
    bh, bl = halves(b)
    return dot(ah, bh, dims) + (dot(ah, bl, dims) + dot(al, bh, dims))


def down_columns(row):
    return jnp.broadcast_to(row, (row.shape[1], row.shape[1])).T


def grid_of(n):
    return (
        lax.broadcasted_iota(jnp.int32, (n, n), 0),
        lax.broadcasted_iota(jnp.int32, (n, n), 1),
    )


def running_sums(rates):
    i, j = grid_of(WIDE)
    upper = jnp.where(i <= j, 1.0, 0.0).astype(BF16)
    high, rest = halves(rates)
    mid = (rates - high.astype(F32) - rest.astype(F32)).astype(BF16)
    return -(dot(high, upper) + (dot(rest, upper) + dot(mid, upper)))


def group_inverses(qs, ks, betas, cums):
    i, j = grid_of(WIDE)
    same = (i // BLOCK) == (j // BLOCK)
    each = range(len(qs))
    rqs, rks, scores, lowers = [], [], [], []
    for q, k, beta, cum in zip(qs, ks, betas, cums):
        qf, kf = q.astype(F32), k.astype(F32)
        rq = lax.rsqrt(jnp.sum(qf * qf, -1, keepdims=True) + EPSILON) * (WIDE**-0.5)
        rk = lax.rsqrt(jnp.sum(kf * kf, -1, keepdims=True) + EPSILON)
        rk_row = jnp.broadcast_to(rk, (WIDE, WIDE)).T
        spread = jnp.where(i >= j, down_columns(cum) - cum, 0.0)
        decay = jnp.exp(spread) * rk_row
        lowers.append(jnp.where(i > j, dot(k, k, NT) * rk * down_columns(beta) * decay, 0.0))
        scores.append(jnp.where(i >= j, dot(q, k, NT) * rq * decay, 0.0))
        rqs.append(rq)
        rks.append((rk, rk_row[:1]))
    powered = [jnp.where(same, -lowers[g], 0.0) for g in each]
    product = [jnp.where(i == j, 1.0, 0.0) + powered[g] for g in each]
    for _ in range(1, (BLOCK - 1).bit_length()):
        powered = [dot_both(powered[g], powered[g]) for g in each]
        product = [product[g] + dot_both(product[g], powered[g]) for g in each]
    crossed = [dot_both(jnp.where(same, 0.0, lowers[g]), product[g]) for g in each]
    inverses = [product[g] - dot_both(product[g], crossed[g]) for g in each]
    return [(inverses[g], scores[g], rqs[g], *rks[g]) for g in each]


def group_terms(q, k, v, beta, cum, inverse, scores, rq, rk, rk_row):
    i, j = grid_of(WIDE)
    cum_col = down_columns(cum)[:, :1]
    last = cum[:, WIDE - 1 :]
    update = dot_left(inverse * beta, v)
    correction = dot_left(inverse * (beta * jnp.exp(cum) * rk_row), k)
    both = jnp.concatenate([update, correction], axis=1)
    moved = dot_right(k, both * (rk * jnp.exp(last - cum_col)), TN)
    shift = moved[:, :WIDE]
    transfer = jnp.where(i == j, jnp.exp(last), 0.0) - moved[:, WIDE:]
    seen = dot_both(scores, both)
    base = seen[:, :WIDE]
    reach = q.astype(F32) * (rq * jnp.exp(cum_col)) - seen[:, WIDE:]
    return shift, transfer, base, reach


def softplus(x):
    return jnp.maximum(x, 0.0) + jnp.log1p(jnp.exp(-jnp.abs(x)))


def dispatch_tables(ids, capacity, experts):
    tokens = ids.shape[1]
    lane = lax.broadcasted_iota(jnp.int32, (tokens, WIDE), 1)
    first = jnp.broadcast_to(ids[0:1].astype(F32), (tokens, tokens)).T.astype(jnp.int32)[:, :WIDE]
    second = jnp.broadcast_to(ids[1:2].astype(F32), (tokens, tokens)).T.astype(jnp.int32)[:, :WIDE]
    one = jnp.where(lane == first, 1.0, 0.0)
    two = jnp.where(lane == second, 1.0, 0.0)
    i, j = grid_of(tokens)
    before = jnp.where(i > j, 1.0, 0.0).astype(BF16)
    rank = dot(before, (one + two).astype(BF16)) + (lane * capacity).astype(F32)
    slot_one = jnp.sum(one * rank, -1, keepdims=True).astype(jnp.int32)
    slot_two = jnp.sum(two * rank, -1, keepdims=True).astype(jnp.int32)
    return slot_one, slot_two


def program_kernel(nz, nx, *refs):
    (
        q_in, k_in, v_in, beta_in, decay_in, ng_in, x_in, gain_in, ids_in, share_in,
        wg_in, wu_in, wd_in, mix_out, ffn_out,
        q_s, k_s, v_s, beta_s, decay_s, ng_s, x_s, gains, ids_s, share_s, wt, wd,
        rows_s, xs, xg, alt, hg, ret, got, base_s, reach_s, total_s, map_out, map_in, state_in, state_out, parts_s,
        load_sem, ready, disp_send, disp_recv, alt_send, alt_recv, x_send, x_recv, hid_send, hid_recv,
        ret_send, ret_recv, g_send, g_recv, w_send, w_recv, s_send, s_recv, m_send, m_recv,
    ) = refs
    grp, z, tp = lax.axis_index("grp"), lax.axis_index("ep"), lax.axis_index("tp")
    x, c = tp // 2, tp % 2
    partner = 2 * x + 1 - c
    tokens, feats = x_s.shape
    capacity = xs.shape[1]
    hid = wg_in.shape[0]
    groups = q_s.shape[0] // WIDE
    sources = nz // 2
    home = 1 - z % 2
    mine = z // 2
    first = z < nz // 4
    corner = jnp.logical_and(z == 0, tp == 0)
    usual = jnp.logical_not(corner)
    below = jnp.logical_and(z > 0, x == 0)
    beside = jnp.logical_and(z == 0, tp > 0)
    proxy = jnp.logical_and(z == 0, tp == 1)
    first_usual = jnp.logical_and(first, usual)
    early = jnp.logical_and(z < nz // 2, usual)
    waits = []

    def remote(src, dst, send, recv, zz, tt):
        return pltpu.make_async_remote_copy(
            src_ref=src, dst_ref=dst, send_sem=send, recv_sem=recv,
            device_id=(grp, zz, tt), device_id_type=MESH,
        )

    def hop(k):
        return min(k, nz - k)

    barrier = pltpu.get_barrier_semaphore()

    def greet(sem, zz, tt):
        pl.semaphore_signal(sem, inc=1, device_id=(grp, zz, tt), device_id_type=MESH)

    around = sorted(range(1, 2 * nx), key=lambda k: -min(k, 2 * nx - k))

    @pl.when(below)
    def _():
        greet(barrier, 0, 0)

    @pl.when(usual)
    def _():
        for dt in around:
            greet(barrier, z, (tp + dt) % (2 * nx))

    for k in range(1, nz):

        @pl.when(jnp.logical_and(z + k < nz, usual))
        def _():
            for core in range(2):
                greet(barrier, (z + k) % nz, 2 * x + core)

    places = [
        (x_in, x_s), (ids_in, ids_s), (beta_in, beta_s), (decay_in, decay_s), (k_in, k_s), (q_in, q_s),
        (v_in, v_s), (gain_in, gains.at[tp]), (share_in, share_s), (ng_in, ng_s),
        (wg_in, wt.at[pl.ds(pl.multiple_of(c * hid, hid), hid), :]),
        (wu_in, wt.at[pl.ds(pl.multiple_of((2 + c) * hid, hid), hid), :]),
        (wd_in, wd.at[c]),
    ]
    loads = [pltpu.make_async_copy(src, dst, load_sem.at[n]) for n, (src, dst) in enumerate(places)]
    for load in loads:
        load.start()

    def mixer_blocks():
        for g in range(groups):
            cut = slice(g * WIDE, (g + 1) * WIDE)
            rows_s[0, g : g + 1, :] = 1.0 / (1.0 + jnp.exp(-beta_s[:, cut]))
            rows_s[1, g : g + 1, :] = softplus(decay_s[:, cut])
        for g in range(groups, 8):
            rows_s[1, g : g + 1, :] = jnp.zeros((1, WIDE), F32)
        rows_s[2] = running_sums(rows_s[1])
        cuts = [slice(g * WIDE, (g + 1) * WIDE) for g in range(groups)]
        qs, ks, vs = [q_s[cut] for cut in cuts], [k_s[cut] for cut in cuts], [v_s[cut] for cut in cuts]
        betas = [rows_s[0, g : g + 1, :] for g in range(groups)]
        cums = [rows_s[2, g : g + 1, :] for g in range(groups)]
        inverses = group_inverses(qs, ks, betas, cums)
        terms = [group_terms(qs[g], ks[g], vs[g], betas[g], cums[g], *inverses[g]) for g in range(groups)]
        total = None
        for cut, (shift, transfer, base, reach) in zip(cuts, terms):
            if total is None:
                total = jnp.concatenate([shift, transfer], axis=1)
            else:
                through = dot_both(reach, total)
                base = base + through[:, :WIDE]
                reach = through[:, WIDE:]
                total = dot_both(transfer, total)
                total = jnp.concatenate([total[:, :WIDE] + shift, total[:, WIDE:]], axis=1)
            base_s[cut, :] = base
            reach_s[cut, :] = reach
        total_s[...] = total
        map_out[...] = total.astype(BF16)

    loads[0].wait()
    loads[1].wait()
    slot_one, slot_two = dispatch_tables(ids_s[...], capacity, nz)
    slots = lax.broadcasted_iota(jnp.int32, (tokens, 2 * tokens), 1)
    chosen = jnp.where((slots == slot_one) | (slots == slot_two), 1.0, 0.0).astype(BF16)
    ordered = dot(chosen, x_s[...], TN).astype(BF16)
    for e in range(nz):
        xs[e] = ordered[e * capacity : (e + 1) * capacity]

    for n in range(2, 7):
        loads[n].wait()

    @pl.when(early)
    def _():
        mixer_blocks()

    missing = jnp.where(jnp.logical_or(below, beside), 1, 0)
    pl.semaphore_wait(barrier, 2 * nx - 1 + jnp.where(corner, 2 * (nz - 1), 2 * z - missing))

    for k in range(nz - 1, 0, -1):

        @pl.when(z >= k)
        def _():
            @pl.when(jnp.logical_or(z > k, x > 0))
            def _():
                greet(ready.at[z], (z + nz - k) % nz, 2 * x)

            greet(ready.at[z], (z + nz - k) % nz, 2 * x + 1)

    row_here = pl.ds(pl.multiple_of(mine * capacity, capacity), capacity)

    def rows_to(e):
        return remote(
            xs.at[e], xg.at[x, c, row_here, :], disp_send.at[0], disp_recv.at[mine, c], e, 2 * x + home
        )

    rows_aside = remote(xs.at[0], alt.at[c, row_here, :], disp_send.at[0], alt_recv.at[mine, c], 0, 1)

    for k in sorted(range(1, nz), key=lambda k: -hop(k)):
        aside = jnp.logical_and(z == k, jnp.logical_and(x == 0, home == 0))

        @pl.when(jnp.logical_or(corner, jnp.logical_and(z >= k, jnp.logical_not(aside))))
        def _():
            rows_to((z + nz - k) % nz).start()

        @pl.when(aside)
        def _():
            rows_aside.start()

    @pl.when(corner)
    def _():
        for dt in around:
            greet(ready.at[0], z, (tp + dt) % (2 * nx))
        for k in sorted(range(1, nz), key=lambda k: -hop(k)):
            for core in range(2):
                greet(ready.at[0], (z + k) % nz, 2 * x + core)

    all_rows = xs.at[pl.ds(0, nz - 1)]
    waits.append((None, remote(all_rows, all_rows, disp_send.at[0], disp_recv.at[0, 0], z, partner)))
    own = remote(xs.at[z], xg.at[x, c, row_here, :], disp_send.at[1], disp_recv.at[mine, c], z, partner)

    @pl.when(home != c)
    def _():
        own.start()

    waits.append((home != c, own))

    @pl.when(home == c)
    def _():
        xg[x, c, row_here, :] = xs[z]

    loads[7].wait()

    def gains_to(dt):
        return remote(gains.at[tp], gains.at[tp], g_send.at[0], g_recv.at[0], z, (tp + dt) % (2 * nx))

    for dt in range(1, 2 * nx):

        @pl.when(jnp.logical_or(z > 0, (tp + dt) % (2 * nx) > 0))
        def _():
            gains_to(dt).start()

    all_gains = gains.at[pl.ds(0, 2 * nx - 1)]
    gains_of_all = remote(all_gains, all_gains, g_send.at[0], g_recv.at[0], z, partner)
    waits.append((None, gains_of_all))
    to_partner = [remote(src, dst, w_send.at[n], w_recv.at[n], z, partner) for n, (src, dst) in enumerate(places[10:])]

    @pl.when(jnp.logical_not(proxy))
    def _():
        for copy in to_partner:
            copy.start()

    for copy in to_partner:
        waits.append((None, copy))

    @pl.when(corner)
    def _():
        mixer_blocks()

    def ready_step(k, condition):
        e = (z + k) % nz

        @pl.when(jnp.logical_and(z + k < nz, condition))
        def _():
            pl.semaphore_wait(ready.at[e], 2)
            rows_to(e).start()

    def away(m, core):
        return jnp.logical_or(2 * m + 1 - c != z, core != c)

    def block(ref, lead, begin, end):
        return ref.at[lead, pl.ds(begin * capacity, (end - begin) * capacity), :]

    def features(chip, begin, end, sem, dx):
        part = xg.at[chip, :, pl.ds(begin * capacity, (end - begin) * capacity), :]
        return remote(part, part, x_send.at[sem], x_recv.at[sem], z, 2 * ((x + dx) % nx) + c)

    def all_features(begin, end, sem, count):
        part = xg.at[pl.ds(0, count), :, pl.ds(begin * capacity, (end - begin) * capacity), :]
        return remote(part, part, x_send.at[sem], x_recv.at[sem], z, partner)

    def all_hidden(begin, end, sem):
        part = hg.at[pl.ds(0, nx - 1), pl.ds(begin * capacity, (end - begin) * capacity), :]
        return remote(part, part, hid_send.at[sem], hid_recv.at[sem], z, partner)

    def hidden_of(chip, begin, end, sem, dx):
        part = block(hg, chip, begin, end)
        return remote(part, part, hid_send.at[sem], hid_recv.at[sem], z, 2 * ((x + dx) % nx) + c)

    farthest = sorted(range(1, nx), key=lambda k: -min(k, nx - k))
    branch = [None]
    gathered = []

    def set_aside(begin, end, sem, dx):
        rows = pl.ds(begin * capacity, (end - begin) * capacity)
        return remote(alt.at[:, rows, :], xg.at[0, :, rows, :], alt_send.at[sem], x_recv.at[sem], z, 2 * dx)

    def gather_aside(begin, end, sem, skip_corner):
        @pl.when(proxy)
        def _():
            for m in range(begin, end):
                for core in range(2):
                    landing = alt.at[core, pl.ds(m * capacity, capacity), :]
                    remote(landing, landing, disp_send.at[0], alt_recv.at[m, core], z, partner).wait_recv()
            for dx in farthest + ([] if skip_corner else [0]):
                set_aside(begin, end, sem, dx).start()

        def gone():
            part = xg.at[:, :, pl.ds(begin * capacity, (end - begin) * capacity), :]
            return remote(part, part, alt_send.at[sem], x_recv.at[sem], z, partner)

        waits.append((proxy, gone))

    def meet_corner(spans=()):
        @pl.when(jnp.logical_or(below, beside))
        def _():
            pl.semaphore_wait(ready.at[0], 1)

        if spans:

            @pl.when(beside)
            def _():
                gains_to(2 * nx - tp).start()

                @pl.when(tp == 1)
                def _():
                    for copy in to_partner:
                        copy.start()
                    for n, (b, e) in enumerate(spans):
                        set_aside(b, e, n, 0).start()

                @pl.when(c == 0)
                def _():
                    for n, (b, e) in enumerate(spans):
                        features(x, b, e, n, nx - x).start()

    def gather_rows(begin, end, sem, skip_corner=False, condition=None):
        def go():
            for m in range(begin, end):
                for core in range(2):
                    landing = xg.at[x, core, pl.ds(m * capacity, capacity), :]
                    arrival = remote(landing, landing, disp_send.at[0], disp_recv.at[m, core], z, partner)

                    @pl.when(away(m, core))
                    def _():
                        arrival.wait_recv()

            for dx in farthest:
                skipped = jnp.logical_and(jnp.logical_and(z == 0, c == 0), (x + dx) % nx == 0)

                @pl.when(jnp.logical_not(jnp.logical_and(skipped, skip_corner)))
                def _():
                    features(x, begin, end, sem, dx).start()

        pl.when(usual if condition is None else jnp.logical_and(usual, condition))(go)
        made = (begin, end, sem, branch[0] is first)
        if made not in gathered:
            gathered.append(made)
            sent = first_usual if branch[0] is first else branch[0]
            waits.append((sent, functools.partial(all_features, begin, end, sem, nx - 1)))

    def make_hidden(begin, end, parts, sem):
        for first_row, last_row, part_sem in parts:
            @pl.when(corner)
            def _():
                all_features(first_row, last_row, part_sem, nx).wait_recv()

            @pl.when(usual)
            def _():
                all_features(first_row, last_row, part_sem, nx - 1).wait_recv()

        rows = slice(begin * capacity, end * capacity)
        acc = jnp.zeros(((end - begin) * capacity, 4 * hid), F32)
        squares = jnp.zeros(((end - begin) * capacity, 1), F32)
        for member in range(2 * nx):
            part = xg[member // 2, member % 2, rows, :].astype(F32)
            squares = squares + jnp.sum(part * part, -1, keepdims=True)
            scaled = (part * gains[member]).astype(BF16)
            acc = acc + dot(scaled, wt[:, member * feats : (member + 1) * feats], NT)
        scale = lax.rsqrt(squares / (feats * 2 * nx) + EPSILON)
        gate = acc[:, : 2 * hid] * scale
        up = acc[:, 2 * hid :] * scale
        hg[x, rows, :] = (gate / (1.0 + jnp.exp(-gate)) * up).astype(BF16)
        for dx in farthest:
            hidden_of(x, begin, end, sem, dx).start()
        waits.append((branch[0], functools.partial(all_hidden, begin, end, sem)))

    rows_all = sources * capacity
    slot_here = pl.ds(pl.multiple_of(z * capacity, capacity), capacity)

    def result(m, core):
        return remote(
            ret.at[core, pl.ds(m * capacity, capacity), :], got.at[slot_here, :],
            ret_send.at[0], ret_recv.at[0], 2 * m + 1 - c, 2 * x + core,
        )

    def give_back(begin, end, sem):
        all_hidden(begin, end, sem).wait_recv()
        rows = slice(begin * capacity, end * capacity)
        hidden = jnp.concatenate([hg[chip, rows, :] for chip in range(nx)], axis=1)
        for core in range(2):
            ret[core, rows, :] = dot(hidden, wd[core]).astype(BF16)
        for m in range(begin, end):
            for core in range(2):

                @pl.when(away(m, core))
                def _():
                    result(m, core).start()

                @pl.when(jnp.logical_not(away(m, core)))
                def _():
                    got[slot_here, :] = ret[core, m * capacity : (m + 1) * capacity, :]

    at_home = home == c
    results_gone = ret.at[:, pl.ds(0, rows_all), :]
    waits.append((jnp.logical_not(at_home), lambda: remote(results_gone, results_gone, ret_send.at[0], ret_recv.at[0], z, partner)))
    some_gone = got.at[pl.ds(0, (2 * sources - 1) * capacity), :]
    waits.append((at_home, lambda: remote(some_gone, some_gone, ret_send.at[0], ret_recv.at[0], z, partner)))

    odd = z % 2 == 1
    send_map = jnp.logical_and(jnp.logical_not(odd), z + 1 < nz)
    own_map = remote(map_out, map_in, m_send.at[0], m_recv.at[0], (z + 1) % nz, tp)
    state_near = remote(state_out, state_in, s_send.at[0], s_recv.at[0], (z + 1) % nz, tp)
    state_far = remote(state_out, state_in, s_send.at[1], s_recv.at[0], (z + 2) % nz, tp)
    waits.append((send_map, own_map))
    waits.append((jnp.logical_and(odd, z + 1 < nz), state_near))
    waits.append((jnp.logical_and(odd, z + 2 < nz), state_far))

    def pass_map(condition):
        @pl.when(jnp.logical_and(condition, send_map))
        def _():
            own_map.start()

    def pass_state():
        @pl.when(z > 1)
        def _():
            state_near.wait_recv()

        @pl.when(z <= 1)
        def _():
            state_in[...] = jnp.zeros_like(state_in)

        @pl.when(odd)
        def _():
            own_map.wait_recv()
            before = map_in[...]
            entering = dot_right(before[:, WIDE:], state_in[...].astype(F32)) + before[:, :WIDE].astype(F32)
            leaving = dot_both(total_s[:, WIDE:], entering) + total_s[:, :WIDE]
            state_out[...] = leaving.astype(BF16)
            high, low = halves(entering)
            parts_s[0] = high
            parts_s[1] = low

            @pl.when(z + 2 < nz)
            def _():
                state_far.start()

            @pl.when(z + 1 < nz)
            def _():
                state_near.start()

        @pl.when(jnp.logical_not(odd))
        def _():
            parts_s[0] = state_in[...]
            parts_s[1] = jnp.zeros_like(state_in)

        for g in range(groups):
            cut = slice(g * WIDE, (g + 1) * WIDE)
            high, low = halves(reach_s[cut, :])
            across = dot(high, parts_s[1]) + dot(low, parts_s[0])
            raw = base_s[cut, :] + (dot(high, parts_s[0]) + across)
            norm = lax.rsqrt(jnp.mean(raw * raw, -1, keepdims=True) + EPSILON)
            mix_out[cut, :] = (raw * norm * ng_s[...]).astype(BF16)

    def weights_here():
        for load in loads[8:]:
            load.wait()
        for n in range(3):
            to_partner[n].wait_recv()
        gains_of_all.wait_recv()

    def marks(*fractions):
        found = [0]
        for part, whole in fractions:
            found.append(max(found[-1], sources * part // whole))
        found.append(sources)
        return [(b, e) for b, e in zip(found[:-1], found[1:]) if e > b]

    branch[0] = first

    @pl.when(first)
    def _():
        steps = iter(range(1, nz))

        def ready_steps(count):
            for k in [k for _, k in zip(range(count), steps)]:
                ready_step(k, usual)

        spans = marks((1, 4), (2, 4), (3, 4), (7, 8))
        last_span = len(spans) - 1
        ready_steps(1)
        pass_map(first)
        ready_steps(nz // 4 - 1)
        waiting = jnp.logical_or(jnp.logical_and(below, c == 1), proxy)
        before, later = list(enumerate(spans[:-1]))[:2], list(enumerate(spans[:-1]))[2:]
        for n, (b, e) in before:
            gather_rows(b, e, n, True, jnp.logical_not(waiting) if n == 0 else None)
            gather_aside(b, e, n, True)
            ready_steps(nz // 4 if n == 0 else nz // 8)
        meet_corner(spans[: len(before)])
        gather_rows(*spans[0], 0, False, waiting)
        ready_steps(nz // 8)
        for n, (b, e) in later:
            gather_rows(b, e, n)
            gather_aside(b, e, n, False)
            ready_steps(1)
        ready_steps(nz)
        weights_here()
        bulk = spans[last_span][0]
        half = spans[min(2, last_span)][0]
        inner = [(b, e, n) for n, (b, e) in enumerate(spans)]
        parts = [(b, e) for b, e in ((0, half), (half, bulk), (bulk, sources)) if e > b]
        given = 0
        for n, (b, e) in enumerate(parts):
            if n == len(parts) - 1 and n > 1:
                give_back(*parts[0], 0)
                given = 1
            make_hidden(b, e, [p for p in inner if b <= p[0] < e], n)
            if n == 0:
                gather_rows(bulk, sources, last_span)
                gather_aside(bulk, sources, last_span, False)
        for n in range(given, len(parts)):
            give_back(*parts[n], n)

    after = jnp.logical_not(first)
    branch[0] = after

    @pl.when(after)
    def _():
        steps = iter(range(1, nz))

        def ready_steps(count):
            for k in [k for _, k in zip(range(count), steps)]:
                ready_step(k, usual)

        spans = marks((1, 8), (2, 8), (4, 8), (6, 8))
        count = len(spans)

        def gather(n, condition=None):
            if n < count:
                gather_rows(*spans[n], n, False, condition)

        def hide(n):
            if n < count:
                make_hidden(*spans[n], [(*spans[n], n)], n)

        def give(n):
            if n < count:
                give_back(*spans[n], n)

        ready_steps(1)
        pass_map(early)
        gather(0)
        ready_steps(2)
        gather(1)
        ready_steps(nz)
        weights_here()
        hide(0)
        hide(1)
        gather(2)
        gather(3, z < nz // 2)
        gather(4, z < nz // 2)
        meet_corner()
        give(0)
        give(1)
        hide(2)
        gather(3, z >= nz // 2)
        give(2)
        gather(4, z >= nz // 2)
        for n in range(3, count):
            hide(n)
        for n in range(3, count):
            give(n)

    @pl.when(z >= nz // 2)
    def _():
        mixer_blocks()

    pass_map(z >= nz // 2)
    pass_state()

    for condition, copy in waits:

        def settle():
            (copy() if callable(copy) else copy).wait_send()

        if condition is None:
            settle()
        else:
            pl.when(condition)(settle)

    shares = share_s[...]
    first_share = jnp.broadcast_to(shares[0:1], (tokens, tokens)).T[:, :1]
    second_share = jnp.broadcast_to(shares[1:2], (tokens, tokens)).T[:, :1]
    weights = jnp.where(slots == slot_one, first_share, 0.0) + jnp.where(slots == slot_two, second_share, 0.0)
    @pl.when(at_home)
    def _():
        most = got.at[pl.ds(0, (nz - 1) * capacity), :]
        remote(most, most, ret_send.at[0], ret_recv.at[0], z, partner).wait_recv()

    @pl.when(jnp.logical_not(at_home))
    def _():
        remote(got, got, ret_send.at[0], ret_recv.at[0], z, partner).wait_recv()

    ffn_out[...] = dot_left(weights, got[...]).astype(BF16)


def body(nz, nx, mix_query, mix_keys, mix_values, beta_in, decay_in, norm_gain, ffn_input, ffn_gain,
         expert_ids, expert_share, w_gate, w_up, w_down):
    length, _, width = mix_query.shape
    tokens, feats = ffn_input.shape
    hid = w_gate.shape[2]
    full = w_gate.shape[1]
    capacity = 2 * tokens // nz
    rows = nz // 2 * capacity
    ff = w_down.shape[1]
    dma = pltpu.SemaphoreType.DMA
    vmem = pltpu.VMEM
    call = pl.pallas_call(
        functools.partial(program_kernel, nz, nx),
        out_shape=(
            pltpu.VMEM((length, width), BF16),
            pltpu.VMEM((tokens, feats), BF16),
        ),
        in_specs=[pl.BlockSpec(memory_space=pl.ANY)] * 13,
        out_specs=[pl.BlockSpec(memory_space=pltpu.VMEM)] * 2,
        scratch_shapes=[
            vmem((length, width), BF16), vmem((length, width), BF16), vmem((length, width), BF16),
            vmem((1, length), F32), vmem((1, length), F32), vmem((1, width), F32),
            vmem((tokens, feats), BF16), vmem((2 * nx, 1, feats), F32),
            vmem((2, tokens), jnp.int32), vmem((2, tokens), F32),
            vmem((4 * hid, full), BF16), vmem((2, ff, feats), BF16),
            vmem((3, 8, width), F32),
            vmem((nz, capacity, feats), BF16),
            vmem((nx, 2, rows, feats), BF16), vmem((2, rows, feats), BF16),
            vmem((nx, rows, 2 * hid), BF16),
            vmem((2, rows, feats), BF16),
            vmem((2 * tokens, feats), BF16),
            vmem((length, width), F32), vmem((length, width), F32), vmem((width, 2 * width), F32),
            vmem((width, 2 * width), BF16), vmem((width, 2 * width), BF16),
            vmem((width, width), BF16), vmem((width, width), BF16), vmem((2, width, width), BF16),
            dma((13,)), pltpu.SemaphoreType.REGULAR((nz,)), dma((2,)), dma((nz // 2, 2)),
            dma((5,)), dma((nz // 2, 2)), dma((5,)), dma((5,)), dma((5,)), dma((5,)),
            dma((1,)), dma((1,)),
            dma((1,)), dma((1,)), dma((3,)), dma((3,)), dma((2,)), dma((1,)), dma((1,)), dma((1,)),
        ],
        compiler_params=pltpu.CompilerParams(collective_id=0, has_side_effects=True),
    )
    mix, ffn = call(
        mix_query.reshape(length, width), mix_keys.reshape(length, width), mix_values.reshape(length, width),
        beta_in, decay_in, norm_gain.reshape(1, width), ffn_input, ffn_gain.reshape(1, feats),
        expert_ids.T, expert_share.T, w_gate[0].T, w_up[0].T, w_down[0],
    )
    return mix.reshape(length, 1, width), ffn


def solution(mesh):
    nz, nx = mesh.shape["ep"], mesh.shape["tp"] // 2
    in_specs = (
        P(("grp", "ep"), "tp", None), P(("grp", "ep"), "tp", None), P(("grp", "ep"), "tp", None),
        P("tp", ("grp", "ep")), P("tp", ("grp", "ep")), P(),
        P(("grp", "ep"), "tp"), P("tp"), P(("grp", "ep"), None), P(("grp", "ep"), None),
        P("ep", None, "tp"), P("ep", None, "tp"), P("ep", None, "tp"),
    )
    out_specs = (P(("grp", "ep"), "tp", None), P(("grp", "ep"), "tp"))
    return jax.shard_map(
        functools.partial(body, nz, nx), mesh=mesh, in_specs=in_specs, out_specs=out_specs, check_vma=False
    )
```

```python
import functools

import jax
import jax.numpy as jnp
from jax import lax
from jax.experimental import pallas as pl
from jax.experimental.pallas import tpu as pltpu
from jax.sharding import PartitionSpec as P

MESH = pl.DeviceIdType.MESH
EPSILON = 1e-06
BLOCK = 64
WIDE = 128
F32 = jnp.float32
BF16 = jnp.bfloat16

NN = ((1,), (0,))
NT = ((1,), (1,))
TN = ((0,), (0,))


def dot(a, b, dims=NN):
    return lax.dot_general(a, b, (dims, ((), ())), preferred_element_type=F32)


def halves(a):
    high = a.astype(BF16)
    return high, (a - high.astype(F32)).astype(BF16)


def dot_left(a, b, dims=NN):
    high, low = halves(a)
    return dot(high, b, dims) + dot(low, b, dims)


def dot_right(a, b, dims=NN):
    high, low = halves(b)
    return dot(a, high, dims) + dot(a, low, dims)


def dot_both(a, b, dims=NN):
    ah, al = halves(a)
    bh, bl = halves(b)
    return dot(ah, bh, dims) + (dot(ah, bl, dims) + dot(al, bh, dims))


def down_columns(row):
    return jnp.broadcast_to(row, (row.shape[1], row.shape[1])).T


def grid_of(n):
    return (
        lax.broadcasted_iota(jnp.int32, (n, n), 0),
        lax.broadcasted_iota(jnp.int32, (n, n), 1),
    )


def running_sums(rates):
    i, j = grid_of(WIDE)
    upper = jnp.where(i <= j, 1.0, 0.0).astype(BF16)
    high, rest = halves(rates)
    mid = (rates - high.astype(F32) - rest.astype(F32)).astype(BF16)
    return -(dot(high, upper) + (dot(rest, upper) + dot(mid, upper)))


def group_inverses(qs, ks, betas, cums):
    i, j = grid_of(WIDE)
    same = (i // BLOCK) == (j // BLOCK)
    each = range(len(qs))
    rqs, rks, scores, lowers = [], [], [], []
    for q, k, beta, cum in zip(qs, ks, betas, cums):
        qf, kf = q.astype(F32), k.astype(F32)
        rq = lax.rsqrt(jnp.sum(qf * qf, -1, keepdims=True) + EPSILON) * (WIDE**-0.5)
        rk = lax.rsqrt(jnp.sum(kf * kf, -1, keepdims=True) + EPSILON)
        rk_row = jnp.broadcast_to(rk, (WIDE, WIDE)).T
        spread = jnp.where(i >= j, down_columns(cum) - cum, 0.0)
        decay = jnp.exp(spread) * rk_row
        lowers.append(jnp.where(i > j, dot(k, k, NT) * rk * down_columns(beta) * decay, 0.0))
        scores.append(jnp.where(i >= j, dot(q, k, NT) * rq * decay, 0.0))
        rqs.append(rq)
        rks.append((rk, rk_row[:1]))
    powered = [jnp.where(same, -lowers[g], 0.0) for g in each]
    product = [jnp.where(i == j, 1.0, 0.0) + powered[g] for g in each]
    for _ in range(1, (BLOCK - 1).bit_length()):
        powered = [dot_both(powered[g], powered[g]) for g in each]
        product = [product[g] + dot_both(product[g], powered[g]) for g in each]
    crossed = [dot_both(jnp.where(same, 0.0, lowers[g]), product[g]) for g in each]
    inverses = [product[g] - dot_both(product[g], crossed[g]) for g in each]
    return [(inverses[g], scores[g], rqs[g], *rks[g]) for g in each]


def group_terms(q, k, v, beta, cum, inverse, scores, rq, rk, rk_row):
    i, j = grid_of(WIDE)
    cum_col = down_columns(cum)[:, :1]
    last = cum[:, WIDE - 1 :]
    update = dot_left(inverse * beta, v)
    correction = dot_left(inverse * (beta * jnp.exp(cum) * rk_row), k)
    both = jnp.concatenate([update, correction], axis=1)
    moved = dot_right(k, both * (rk * jnp.exp(last - cum_col)), TN)
    shift = moved[:, :WIDE]
    transfer = jnp.where(i == j, jnp.exp(last), 0.0) - moved[:, WIDE:]
    seen = dot_both(scores, both)
    base = seen[:, :WIDE]
    reach = q.astype(F32) * (rq * jnp.exp(cum_col)) - seen[:, WIDE:]
    return shift, transfer, base, reach


def softplus(x):
    return jnp.maximum(x, 0.0) + jnp.log1p(jnp.exp(-jnp.abs(x)))


def dispatch_tables(ids, capacity, experts):
    tokens = ids.shape[1]
    lane = lax.broadcasted_iota(jnp.int32, (tokens, WIDE), 1)
    first = jnp.broadcast_to(ids[0:1].astype(F32), (tokens, tokens)).T.astype(jnp.int32)[:, :WIDE]
    second = jnp.broadcast_to(ids[1:2].astype(F32), (tokens, tokens)).T.astype(jnp.int32)[:, :WIDE]
    one = jnp.where(lane == first, 1.0, 0.0)
    two = jnp.where(lane == second, 1.0, 0.0)
    i, j = grid_of(tokens)
    before = jnp.where(i > j, 1.0, 0.0).astype(BF16)
    rank = dot(before, (one + two).astype(BF16)) + (lane * capacity).astype(F32)
    slot_one = jnp.sum(one * rank, -1, keepdims=True).astype(jnp.int32)
    slot_two = jnp.sum(two * rank, -1, keepdims=True).astype(jnp.int32)
    return slot_one, slot_two


def program_kernel(nz, nx, *refs):
    (
        q_in, k_in, v_in, beta_in, decay_in, ng_in, x_in, gain_in, ids_in, share_in,
        wg_in, wu_in, wd_in, mix_out, ffn_out,
        q_s, k_s, v_s, beta_s, decay_s, ng_s, x_s, gains, ids_s, share_s, wt, wd,
        rows_s, xs, xg, alt, hg, ret, got, base_s, reach_s, total_s, map_out, map_in, state_in, state_out, parts_s,
        load_sem, ready, disp_send, disp_recv, alt_send, alt_recv, x_send, x_recv, hid_send, hid_recv,
        ret_send, ret_recv, g_send, g_recv, w_send, w_recv, s_send, s_recv, m_send, m_recv,
    ) = refs
    grp, z, tp = lax.axis_index("grp"), lax.axis_index("ep"), lax.axis_index("tp")
    x, c = tp // 2, tp % 2
    partner = 2 * x + 1 - c
    tokens, feats = x_s.shape
    capacity = xs.shape[1]
    hid = wg_in.shape[0]
    groups = q_s.shape[0] // WIDE
    sources = nz // 2
    home = 1 - z % 2
    mine = z // 2
    first = z < nz // 4
    corner = jnp.logical_and(z == 0, tp == 0)
    usual = jnp.logical_not(corner)
    below = jnp.logical_and(z > 0, x == 0)
    beside = jnp.logical_and(z == 0, tp > 0)
    proxy = jnp.logical_and(z == 0, tp == 1)
    first_usual = jnp.logical_and(first, usual)
    early = jnp.logical_and(z < nz // 2, usual)
    waits = []

    def remote(src, dst, send, recv, zz, tt):
        return pltpu.make_async_remote_copy(
            src_ref=src, dst_ref=dst, send_sem=send, recv_sem=recv,
            device_id=(grp, zz, tt), device_id_type=MESH,
        )

    def hop(k):
        return min(k, nz - k)

    barrier = pltpu.get_barrier_semaphore()

    def greet(sem, zz, tt):
        pl.semaphore_signal(sem, inc=1, device_id=(grp, zz, tt), device_id_type=MESH)

    around = sorted(range(1, 2 * nx), key=lambda k: -min(k, 2 * nx - k))

    @pl.when(below)
    def _():
        greet(barrier, 0, 0)

    @pl.when(usual)
    def _():
        for dt in around:
            greet(barrier, z, (tp + dt) % (2 * nx))

    for k in range(1, nz):

        @pl.when(jnp.logical_and(z + k < nz, usual))
        def _():
            for core in range(2):
                greet(barrier, (z + k) % nz, 2 * x + core)

    places = [
        (x_in, x_s), (ids_in, ids_s), (beta_in, beta_s), (decay_in, decay_s), (k_in, k_s), (q_in, q_s),
        (v_in, v_s), (gain_in, gains.at[tp]), (share_in, share_s), (ng_in, ng_s),
        (wg_in, wt.at[pl.ds(pl.multiple_of(c * hid, hid), hid), :]),
        (wu_in, wt.at[pl.ds(pl.multiple_of((2 + c) * hid, hid), hid), :]),
        (wd_in, wd.at[c]),
    ]
    loads = [pltpu.make_async_copy(src, dst, load_sem.at[n]) for n, (src, dst) in enumerate(places)]
    for load in loads:
        load.start()

    def mixer_blocks():
        for g in range(groups):
            cut = slice(g * WIDE, (g + 1) * WIDE)
            rows_s[0, g : g + 1, :] = 1.0 / (1.0 + jnp.exp(-beta_s[:, cut]))
            rows_s[1, g : g + 1, :] = softplus(decay_s[:, cut])
        for g in range(groups, 8):
            rows_s[1, g : g + 1, :] = jnp.zeros((1, WIDE), F32)
        rows_s[2] = running_sums(rows_s[1])
        cuts = [slice(g * WIDE, (g + 1) * WIDE) for g in range(groups)]
        qs, ks, vs = [q_s[cut] for cut in cuts], [k_s[cut] for cut in cuts], [v_s[cut] for cut in cuts]
        betas = [rows_s[0, g : g + 1, :] for g in range(groups)]
        cums = [rows_s[2, g : g + 1, :] for g in range(groups)]
        inverses = group_inverses(qs, ks, betas, cums)
        terms = [group_terms(qs[g], ks[g], vs[g], betas[g], cums[g], *inverses[g]) for g in range(groups)]
        total = None
        for cut, (shift, transfer, base, reach) in zip(cuts, terms):
            if total is None:
                total = jnp.concatenate([shift, transfer], axis=1)
            else:
                through = dot_both(reach, total)
                base = base + through[:, :WIDE]
                reach = through[:, WIDE:]
                total = dot_both(transfer, total)
                total = jnp.concatenate([total[:, :WIDE] + shift, total[:, WIDE:]], axis=1)
            base_s[cut, :] = base
            reach_s[cut, :] = reach
        total_s[...] = total
        map_out[...] = total.astype(BF16)

    loads[0].wait()
    loads[1].wait()
    slot_one, slot_two = dispatch_tables(ids_s[...], capacity, nz)
    slots = lax.broadcasted_iota(jnp.int32, (tokens, 2 * tokens), 1)
    chosen = jnp.where((slots == slot_one) | (slots == slot_two), 1.0, 0.0).astype(BF16)
    ordered = dot(chosen, x_s[...], TN).astype(BF16)
    for e in range(nz):
        xs[e] = ordered[e * capacity : (e + 1) * capacity]

    for n in range(2, 7):
        loads[n].wait()

    @pl.when(early)
    def _():
        mixer_blocks()

    missing = jnp.where(jnp.logical_or(below, beside), 1, 0)
    pl.semaphore_wait(barrier, 2 * nx - 1 + jnp.where(corner, 2 * (nz - 1), 2 * z - missing))

    for k in range(nz - 1, 0, -1):

        @pl.when(z >= k)
        def _():
            @pl.when(jnp.logical_or(z > k, x > 0))
            def _():
                greet(ready.at[z], (z + nz - k) % nz, 2 * x)

            greet(ready.at[z], (z + nz - k) % nz, 2 * x + 1)

    row_here = pl.ds(pl.multiple_of(mine * capacity, capacity), capacity)

    def rows_to(e):
        return remote(
            xs.at[e], xg.at[x, c, row_here, :], disp_send.at[0], disp_recv.at[mine, c], e, 2 * x + home
        )

    rows_aside = remote(xs.at[0], alt.at[c, row_here, :], disp_send.at[0], alt_recv.at[mine, c], 0, 1)

    for k in sorted(range(1, nz), key=lambda k: -hop(k)):
        aside = jnp.logical_and(z == k, jnp.logical_and(x == 0, home == 0))

        @pl.when(jnp.logical_or(corner, jnp.logical_and(z >= k, jnp.logical_not(aside))))
        def _():
            rows_to((z + nz - k) % nz).start()

        @pl.when(aside)
        def _():
            rows_aside.start()

    @pl.when(corner)
    def _():
        for dt in around:
            greet(ready.at[0], z, (tp + dt) % (2 * nx))
        for k in sorted(range(1, nz), key=lambda k: -hop(k)):
            for core in range(2):
                greet(ready.at[0], (z + k) % nz, 2 * x + core)

    all_rows = xs.at[pl.ds(0, nz - 1)]
    waits.append((None, remote(all_rows, all_rows, disp_send.at[0], disp_recv.at[0, 0], z, partner)))
    own = remote(xs.at[z], xg.at[x, c, row_here, :], disp_send.at[1], disp_recv.at[mine, c], z, partner)

    @pl.when(home != c)
    def _():
        own.start()

    waits.append((home != c, own))

    @pl.when(home == c)
    def _():
        xg[x, c, row_here, :] = xs[z]

    loads[7].wait()

    def gains_to(dt):
        return remote(gains.at[tp], gains.at[tp], g_send.at[0], g_recv.at[0], z, (tp + dt) % (2 * nx))

    for dt in range(1, 2 * nx):

        @pl.when(jnp.logical_or(z > 0, (tp + dt) % (2 * nx) > 0))
        def _():
            gains_to(dt).start()

    all_gains = gains.at[pl.ds(0, 2 * nx - 1)]
    gains_of_all = remote(all_gains, all_gains, g_send.at[0], g_recv.at[0], z, partner)
    waits.append((None, gains_of_all))
    to_partner = [remote(src, dst, w_send.at[n], w_recv.at[n], z, partner) for n, (src, dst) in enumerate(places[10:])]

    @pl.when(jnp.logical_not(proxy))
    def _():
        for copy in to_partner:
            copy.start()

    for copy in to_partner:
        waits.append((None, copy))

    @pl.when(corner)
    def _():
        mixer_blocks()

    def ready_step(k, condition):
        e = (z + k) % nz

        @pl.when(jnp.logical_and(z + k < nz, condition))
        def _():
            pl.semaphore_wait(ready.at[e], 2)
            rows_to(e).start()

    def away(m, core):
        return jnp.logical_or(2 * m + 1 - c != z, core != c)

    def block(ref, lead, begin, end):
        return ref.at[lead, pl.ds(begin * capacity, (end - begin) * capacity), :]

    def features(chip, begin, end, sem, dx):
        part = xg.at[chip, :, pl.ds(begin * capacity, (end - begin) * capacity), :]
        return remote(part, part, x_send.at[sem], x_recv.at[sem], z, 2 * ((x + dx) % nx) + c)

    def all_features(begin, end, sem, count):
        part = xg.at[pl.ds(0, count), :, pl.ds(begin * capacity, (end - begin) * capacity), :]
        return remote(part, part, x_send.at[sem], x_recv.at[sem], z, partner)

    def all_hidden(begin, end, sem):
        part = hg.at[pl.ds(0, nx - 1), pl.ds(begin * capacity, (end - begin) * capacity), :]
        return remote(part, part, hid_send.at[sem], hid_recv.at[sem], z, partner)

    def hidden_of(chip, begin, end, sem, dx):
        part = block(hg, chip, begin, end)
        return remote(part, part, hid_send.at[sem], hid_recv.at[sem], z, 2 * ((x + dx) % nx) + c)

    farthest = sorted(range(1, nx), key=lambda k: -min(k, nx - k))
    branch = [None]
    gathered = []

    def set_aside(begin, end, sem, dx):
        rows = pl.ds(begin * capacity, (end - begin) * capacity)
        return remote(alt.at[:, rows, :], xg.at[0, :, rows, :], alt_send.at[sem], x_recv.at[sem], z, 2 * dx)

    def gather_aside(begin, end, sem, skip_corner):
        @pl.when(proxy)
        def _():
            for m in range(begin, end):
                for core in range(2):
                    landing = alt.at[core, pl.ds(m * capacity, capacity), :]
                    remote(landing, landing, disp_send.at[0], alt_recv.at[m, core], z, partner).wait_recv()
            for dx in farthest + ([] if skip_corner else [0]):
                set_aside(begin, end, sem, dx).start()

        def gone():
            part = xg.at[:, :, pl.ds(begin * capacity, (end - begin) * capacity), :]
            return remote(part, part, alt_send.at[sem], x_recv.at[sem], z, partner)

        waits.append((proxy, gone))

    def meet_corner(spans=()):
        @pl.when(jnp.logical_or(below, beside))
        def _():
            pl.semaphore_wait(ready.at[0], 1)

        if spans:

            @pl.when(beside)
            def _():
                gains_to(2 * nx - tp).start()

                @pl.when(tp == 1)
                def _():
                    for copy in to_partner:
                        copy.start()
                    for n, (b, e) in enumerate(spans):
                        set_aside(b, e, n, 0).start()

                @pl.when(c == 0)
                def _():
                    for n, (b, e) in enumerate(spans):
                        features(x, b, e, n, nx - x).start()

    def gather_rows(begin, end, sem, skip_corner=False, condition=None):
        def go():
            for m in range(begin, end):
                for core in range(2):
                    landing = xg.at[x, core, pl.ds(m * capacity, capacity), :]
                    arrival = remote(landing, landing, disp_send.at[0], disp_recv.at[m, core], z, partner)

                    @pl.when(away(m, core))
                    def _():
                        arrival.wait_recv()

            for dx in farthest:
                skipped = jnp.logical_and(jnp.logical_and(z == 0, c == 0), (x + dx) % nx == 0)

                @pl.when(jnp.logical_not(jnp.logical_and(skipped, skip_corner)))
                def _():
                    features(x, begin, end, sem, dx).start()

        pl.when(usual if condition is None else jnp.logical_and(usual, condition))(go)
        made = (begin, end, sem, branch[0] is first)
        if made not in gathered:
            gathered.append(made)
            sent = first_usual if branch[0] is first else branch[0]
            waits.append((sent, functools.partial(all_features, begin, end, sem, nx - 1)))

    def make_hidden(begin, end, parts, sem):
        for first_row, last_row, part_sem in parts:
            @pl.when(corner)
            def _():
                all_features(first_row, last_row, part_sem, nx).wait_recv()

            @pl.when(usual)
            def _():
                all_features(first_row, last_row, part_sem, nx - 1).wait_recv()

        rows = slice(begin * capacity, end * capacity)
        acc = jnp.zeros(((end - begin) * capacity, 4 * hid), F32)
        squares = jnp.zeros(((end - begin) * capacity, 1), F32)
        for member in range(2 * nx):
            part = xg[member // 2, member % 2, rows, :].astype(F32)
            squares = squares + jnp.sum(part * part, -1, keepdims=True)
            scaled = (part * gains[member]).astype(BF16)
            acc = acc + dot(scaled, wt[:, member * feats : (member + 1) * feats], NT)
        scale = lax.rsqrt(squares / (feats * 2 * nx) + EPSILON)
        gate = acc[:, : 2 * hid] * scale
        up = acc[:, 2 * hid :] * scale
        hg[x, rows, :] = (gate / (1.0 + jnp.exp(-gate)) * up).astype(BF16)
        for dx in farthest:
            hidden_of(x, begin, end, sem, dx).start()
        waits.append((branch[0], functools.partial(all_hidden, begin, end, sem)))

    rows_all = sources * capacity
    slot_here = pl.ds(pl.multiple_of(z * capacity, capacity), capacity)

    def result(m, core):
        return remote(
            ret.at[core, pl.ds(m * capacity, capacity), :], got.at[slot_here, :],
            ret_send.at[0], ret_recv.at[0], 2 * m + 1 - c, 2 * x + core,
        )

    def give_back(begin, end, sem):
        all_hidden(begin, end, sem).wait_recv()
        rows = slice(begin * capacity, end * capacity)
        hidden = jnp.concatenate([hg[chip, rows, :] for chip in range(nx)], axis=1)
        for core in range(2):
            ret[core, rows, :] = dot(hidden, wd[core]).astype(BF16)
        for m in range(begin, end):
            for core in range(2):

                @pl.when(away(m, core))
                def _():
                    result(m, core).start()

                @pl.when(jnp.logical_not(away(m, core)))
                def _():
                    got[slot_here, :] = ret[core, m * capacity : (m + 1) * capacity, :]

    at_home = home == c
    results_gone = ret.at[:, pl.ds(0, rows_all), :]
    waits.append((jnp.logical_not(at_home), lambda: remote(results_gone, results_gone, ret_send.at[0], ret_recv.at[0], z, partner)))
    some_gone = got.at[pl.ds(0, (2 * sources - 1) * capacity), :]
    waits.append((at_home, lambda: remote(some_gone, some_gone, ret_send.at[0], ret_recv.at[0], z, partner)))

    odd = z % 2 == 1
    send_map = jnp.logical_and(jnp.logical_not(odd), z + 1 < nz)
    own_map = remote(map_out, map_in, m_send.at[0], m_recv.at[0], (z + 1) % nz, tp)
    state_near = remote(state_out, state_in, s_send.at[0], s_recv.at[0], (z + 1) % nz, tp)
    state_far = remote(state_out, state_in, s_send.at[1], s_recv.at[0], (z + 2) % nz, tp)
    waits.append((send_map, own_map))
    waits.append((jnp.logical_and(odd, z + 1 < nz), state_near))
    waits.append((jnp.logical_and(odd, z + 2 < nz), state_far))

    def pass_map(condition):
        @pl.when(jnp.logical_and(condition, send_map))
        def _():
            own_map.start()

    def pass_state():
        @pl.when(z > 1)
        def _():
            state_near.wait_recv()

        @pl.when(z <= 1)
        def _():
            state_in[...] = jnp.zeros_like(state_in)

        @pl.when(odd)
        def _():
            own_map.wait_recv()
            before = map_in[...]
            entering = dot_right(before[:, WIDE:], state_in[...].astype(F32)) + before[:, :WIDE].astype(F32)
            leaving = dot_both(total_s[:, WIDE:], entering) + total_s[:, :WIDE]
            state_out[...] = leaving.astype(BF16)
            high, low = halves(entering)
            parts_s[0] = high
            parts_s[1] = low

            @pl.when(z + 2 < nz)
            def _():
                state_far.start()

            @pl.when(z + 1 < nz)
            def _():
                state_near.start()

        @pl.when(jnp.logical_not(odd))
        def _():
            parts_s[0] = state_in[...]
            parts_s[1] = jnp.zeros_like(state_in)

        for g in range(groups):
            cut = slice(g * WIDE, (g + 1) * WIDE)
            high, low = halves(reach_s[cut, :])
            across = dot(high, parts_s[1]) + dot(low, parts_s[0])
            raw = base_s[cut, :] + (dot(high, parts_s[0]) + across)
            norm = lax.rsqrt(jnp.mean(raw * raw, -1, keepdims=True) + EPSILON)
            mix_out[cut, :] = (raw * norm * ng_s[...]).astype(BF16)

    def weights_here():
        for load in loads[8:]:
            load.wait()
        for n in range(3):
            to_partner[n].wait_recv()
        gains_of_all.wait_recv()

    def marks(*fractions):
        found = [0]
        for part, whole in fractions:
            found.append(max(found[-1], sources * part // whole))
        found.append(sources)
        return [(b, e) for b, e in zip(found[:-1], found[1:]) if e > b]

    branch[0] = first

    @pl.when(first)
    def _():
        steps = iter(range(1, nz))

        def ready_steps(count):
            for k in [k for _, k in zip(range(count), steps)]:
                ready_step(k, usual)

        spans = marks((1, 4), (2, 4), (3, 4), (7, 8))
        last_span = len(spans) - 1
        ready_steps(1)
        pass_map(first)
        ready_steps(nz // 4 - 1)
        waiting = jnp.logical_or(jnp.logical_and(below, c == 1), proxy)
        before, later = list(enumerate(spans[:-1]))[:2], list(enumerate(spans[:-1]))[2:]
        for n, (b, e) in before:
            gather_rows(b, e, n, True, jnp.logical_not(waiting) if n == 0 else None)
            gather_aside(b, e, n, True)
            ready_steps(nz // 4 if n == 0 else nz // 8)
        meet_corner(spans[: len(before)])
        gather_rows(*spans[0], 0, False, waiting)
        ready_steps(nz // 8)
        for n, (b, e) in later:
            gather_rows(b, e, n)
            gather_aside(b, e, n, False)
            ready_steps(1)
        ready_steps(nz)
        weights_here()
        bulk = spans[last_span][0]
        half = spans[min(2, last_span)][0]
        inner = [(b, e, n) for n, (b, e) in enumerate(spans)]
        parts = [(b, e) for b, e in ((0, half), (half, bulk), (bulk, sources)) if e > b]
        for n, (b, e) in enumerate(parts):
            make_hidden(b, e, [p for p in inner if b <= p[0] < e], n)
            if n == 0:
                gather_rows(bulk, sources, last_span)
                gather_aside(bulk, sources, last_span, False)
                give_back(*parts[0], 0)
        for n in range(1, len(parts)):
            give_back(*parts[n], n)

    after = jnp.logical_not(first)
    branch[0] = after

    @pl.when(after)
    def _():
        steps = iter(range(1, nz))

        def ready_steps(count):
            for k in [k for _, k in zip(range(count), steps)]:
                ready_step(k, usual)

        spans = marks((1, 8), (2, 8), (4, 8), (6, 8))
        count = len(spans)

        def gather(n, condition=None):
            if n < count:
                gather_rows(*spans[n], n, False, condition)

        def hide(n):
            if n < count:
                make_hidden(*spans[n], [(*spans[n], n)], n)

        def give(n):
            if n < count:
                give_back(*spans[n], n)

        ready_steps(1)
        pass_map(early)
        gather(0)
        ready_steps(2)
        gather(1)
        ready_steps(nz)
        weights_here()
        hide(0)
        hide(1)
        gather(2)
        gather(3, z < nz // 2)
        gather(4, z < nz // 2)
        meet_corner()
        give(0)
        give(1)
        hide(2)
        gather(3, z >= nz // 2)
        pl.when(z >= nz // 2)(lambda: give(2))
        gather(4, z >= nz // 2)
        for n in range(3, count):
            hide(n)
        pl.when(z < nz // 2)(lambda: give(2))
        for n in range(3, count):
            give(n)

    @pl.when(z >= nz // 2)
    def _():
        mixer_blocks()

    pass_map(z >= nz // 2)
    pass_state()

    for condition, copy in waits:

        def settle():
            (copy() if callable(copy) else copy).wait_send()

        if condition is None:
            settle()
        else:
            pl.when(condition)(settle)

    shares = share_s[...]
    first_share = jnp.broadcast_to(shares[0:1], (tokens, tokens)).T[:, :1]
    second_share = jnp.broadcast_to(shares[1:2], (tokens, tokens)).T[:, :1]
    weights = jnp.where(slots == slot_one, first_share, 0.0) + jnp.where(slots == slot_two, second_share, 0.0)
    @pl.when(at_home)
    def _():
        most = got.at[pl.ds(0, (nz - 1) * capacity), :]
        remote(most, most, ret_send.at[0], ret_recv.at[0], z, partner).wait_recv()

    @pl.when(jnp.logical_not(at_home))
    def _():
        remote(got, got, ret_send.at[0], ret_recv.at[0], z, partner).wait_recv()

    ffn_out[...] = dot_left(weights, got[...]).astype(BF16)


def body(nz, nx, mix_query, mix_keys, mix_values, beta_in, decay_in, norm_gain, ffn_input, ffn_gain,
         expert_ids, expert_share, w_gate, w_up, w_down):
    length, _, width = mix_query.shape
    tokens, feats = ffn_input.shape
    hid = w_gate.shape[2]
    full = w_gate.shape[1]
    capacity = 2 * tokens // nz
    rows = nz // 2 * capacity
    ff = w_down.shape[1]
    dma = pltpu.SemaphoreType.DMA
    vmem = pltpu.VMEM
    call = pl.pallas_call(
        functools.partial(program_kernel, nz, nx),
        out_shape=(
            pltpu.VMEM((length, width), BF16),
            pltpu.VMEM((tokens, feats), BF16),
        ),
        in_specs=[pl.BlockSpec(memory_space=pl.ANY)] * 13,
        out_specs=[pl.BlockSpec(memory_space=pltpu.VMEM)] * 2,
        scratch_shapes=[
            vmem((length, width), BF16), vmem((length, width), BF16), vmem((length, width), BF16),
            vmem((1, length), F32), vmem((1, length), F32), vmem((1, width), F32),
            vmem((tokens, feats), BF16), vmem((2 * nx, 1, feats), F32),
            vmem((2, tokens), jnp.int32), vmem((2, tokens), F32),
            vmem((4 * hid, full), BF16), vmem((2, ff, feats), BF16),
            vmem((3, 8, width), F32),
            vmem((nz, capacity, feats), BF16),
            vmem((nx, 2, rows, feats), BF16), vmem((2, rows, feats), BF16),
            vmem((nx, rows, 2 * hid), BF16),
            vmem((2, rows, feats), BF16),
            vmem((2 * tokens, feats), BF16),
            vmem((length, width), F32), vmem((length, width), F32), vmem((width, 2 * width), F32),
            vmem((width, 2 * width), BF16), vmem((width, 2 * width), BF16),
            vmem((width, width), BF16), vmem((width, width), BF16), vmem((2, width, width), BF16),
            dma((13,)), pltpu.SemaphoreType.REGULAR((nz,)), dma((2,)), dma((nz // 2, 2)),
            dma((5,)), dma((nz // 2, 2)), dma((5,)), dma((5,)), dma((5,)), dma((5,)),
            dma((1,)), dma((1,)),
            dma((1,)), dma((1,)), dma((3,)), dma((3,)), dma((2,)), dma((1,)), dma((1,)), dma((1,)),
        ],
        compiler_params=pltpu.CompilerParams(collective_id=0, has_side_effects=True),
    )
    mix, ffn = call(
        mix_query.reshape(length, width), mix_keys.reshape(length, width), mix_values.reshape(length, width),
        beta_in, decay_in, norm_gain.reshape(1, width), ffn_input, ffn_gain.reshape(1, feats),
        expert_ids.T, expert_share.T, w_gate[0].T, w_up[0].T, w_down[0],
    )
    return mix.reshape(length, 1, width), ffn


def solution(mesh):
    nz, nx = mesh.shape["ep"], mesh.shape["tp"] // 2
    in_specs = (
        P(("grp", "ep"), "tp", None), P(("grp", "ep"), "tp", None), P(("grp", "ep"), "tp", None),
        P("tp", ("grp", "ep")), P("tp", ("grp", "ep")), P(),
        P(("grp", "ep"), "tp"), P("tp"), P(("grp", "ep"), None), P(("grp", "ep"), None),
        P("ep", None, "tp"), P("ep", None, "tp"), P("ep", None, "tp"),
    )
    out_specs = (P(("grp", "ep"), "tp", None), P(("grp", "ep"), "tp"))
    return jax.shard_map(
        functools.partial(body, nz, nx), mesh=mesh, in_specs=in_specs, out_specs=out_specs, check_vma=False
    )
```
